32 devices in a mesh: grp: 2 (over y), sp: 4 (over z), tp: 4 (over x, core).
Axes of the slice: x: 2, y: 2, z: 4, core: 2. Of those that a mesh axis runs over, the one named last changes fastest.
Arguments:
- tokens: bfloat16 [4096, 4096], P(('grp', 'sp', 'tp')), parts along dimension 0, may hold values from -6 to 6
- norm_gain: float32 [4096], replicated, may hold values from 0.1 to 1.9
- query_diff: bfloat16 [4096, 2048], P('sp', 'tp'), may hold values from -1.25 to 1.25
- key_diff: bfloat16 [4096, 2048], P('sp', 'tp'), may hold values from -1.25 to 1.25
- value_diff: bfloat16 [4096, 2048], P('sp', 'tp'), may hold values from -0.09375 to 0.09375
- lam: float32 [8], P('tp'), may hold values from 0.3 to 0.8
- output_norm_gain: float32 [256], replicated, may hold values from 0.1 to 1.9
- query_win: bfloat16 [4096, 2048], P('sp', 'tp'), may hold values from -1.25 to 1.25
- keyval_win: bfloat16 [4, 4096, 256], P(None, 'sp'), may hold values from -1.25 to 1.25
- sink: float32 [16], P('tp'), may hold values from 4 to 7
- proj_diff: bfloat16 [2048, 4096], P('tp'), may hold values from -0.125 to 0.125
- proj_win: bfloat16 [2048, 4096], P('tp'), may hold values from -0.79296875 to 0.79296875
Outputs:
- mixed: bfloat16 [4096, 4096], P(('grp', 'sp', 'tp')), parts along dimension 0
The draws below stay inside these ranges and needn't reach their ends.
There are 2 independent parts, one for each index of `grp`. The reference program is written for one: setup_inputs(seed, part) draws one part's arguments, and reference() takes and returns one part's arrays. A program takes and returns all parts, laid end to end along the dimension named above; an argument that names none is the same for every part. Nothing has to cross between parts.
All inputs are finite; a program needn't handle non-finite values.
Results may differ from the reference program's by a relative error of at most 0.015.
Values may be sent and summed in bfloat16 or wider, within the bound.
No kernel may reach another device: no remote copies, remote signals or barrier semaphores. Data moves between devices by JAX's collectives and lax.ppermute only.
A program may use at most 128 MiB of HBM per device.

```python
import math
import jax
import jax.numpy as jnp
from jax import lax

D = 4096
HEAD = 128
DIFF_HEADS = 8
WIN_HEADS = 16
KV_HEADS = 4
WINDOW = 128
VDIM = 256
SEQ = 2048


def draw_tokens(key, part):
    base = jnp.clip(jax.random.normal(key, (SEQ, D), jnp.float32), -6.0, 6.0)
    return base.astype(jnp.bfloat16)


def diff_pair(key):
    scale = 1.3 * D ** (-0.5)
    width = DIFF_HEADS * 2 * HEAD
    first = jnp.clip(jax.random.normal(jax.random.fold_in(key, 11), (D, width), jnp.float32), -4.0, 4.0) * scale
    second = jnp.clip(jax.random.normal(jax.random.fold_in(key, 12), (D, width), jnp.float32), -4.0, 4.0) * scale
    return (first, second)


def draw_query_diff(key, part):
    return diff_pair(key)[0].astype(jnp.bfloat16)


def draw_key_diff(key, part):
    return diff_pair(key)[1].astype(jnp.bfloat16)


def window_pair(key):
    scale = 1.3 * D ** (-0.5)
    keys = jnp.clip(jax.random.normal(jax.random.fold_in(key, 21), (KV_HEADS, D, HEAD), jnp.float32), -4.0, 4.0) * scale
    values = jnp.clip(jax.random.normal(jax.random.fold_in(key, 22), (KV_HEADS, D, HEAD), jnp.float32), -4.0, 4.0) * D ** (-0.5)
    queries = jnp.clip(jax.random.normal(jax.random.fold_in(key, 23), (D, WIN_HEADS * HEAD), jnp.float32), -4.0, 4.0) * scale
    return (queries, jnp.concatenate([keys, values], axis=2))


def draw_query_win(key, part):
    return window_pair(key)[0].astype(jnp.bfloat16)


def draw_keyval_win(key, part):
    return window_pair(key)[1].astype(jnp.bfloat16)


def shard_levels(rng, dims, split, least, top_value):
    level = 1.0
    for position, parts in split:
        steps = jax.random.uniform(jax.random.fold_in(jax.random.fold_in(rng, 6), position), (parts,), jnp.float32, least / len(split), top_value / len(split))
        level = level * jnp.repeat(jnp.exp(steps), dims[position] // parts).reshape((-1,) + (1,) * (len(dims) - 1 - position))
    return level


def scatter_about(rng, dims, scale, limit, shards=(), kind=jnp.bfloat16):
    values = scale * jax.random.normal(rng, dims, jnp.float32)
    if shards:
        values = values * shard_levels(rng, dims, shards, -0.22, 0.18)
    return jnp.clip(values, -limit, limit).astype(kind)


def setup_inputs(seed: int = 0, part: int = 0) -> dict:
    key_of = jax.random.split(jax.random.key(seed), 13)
    part_splits = jax.random.split(jax.random.fold_in(key_of[12], part), 13)
    return {
        "tokens": draw_tokens(jax.random.fold_in(jax.random.fold_in(key_of[12], part), 71), part),
        "norm_gain": jnp.clip(1.0 + 0.18 * jax.random.normal(key_of[1], (D,), jnp.float32), 0.1, 1.9),
        "query_diff": draw_query_diff(jax.random.fold_in(key_of[12], 71), part),
        "key_diff": draw_key_diff(jax.random.fold_in(key_of[12], 71), part),
        "value_diff": scatter_about(key_of[4], (D, DIFF_HEADS * VDIM), D ** -0.5, 0.09375, ((0, 4), (1, 4))),
        "lam": jnp.clip(0.3 + 0.5 * jax.random.uniform(key_of[5], (DIFF_HEADS,), jnp.float32) ** shard_levels(key_of[5], (DIFF_HEADS,), ((0, 4),), -0.2, 0.2), 0.3, 0.8),
        "output_norm_gain": jnp.clip(1.0 + 0.18 * jax.random.normal(key_of[6], (VDIM,), jnp.float32), 0.1, 1.9),
        "query_win": draw_query_win(jax.random.fold_in(key_of[12], 71), part),
        "keyval_win": draw_keyval_win(jax.random.fold_in(key_of[12], 71), part),
        "sink": jnp.clip(4.0 + 3.0 * jax.random.uniform(key_of[9], (WIN_HEADS,), jnp.float32) ** shard_levels(key_of[9], (WIN_HEADS,), ((0, 4),), -0.2, 0.2), 4.0, 7.0),
        "proj_diff": scatter_about(key_of[10], (DIFF_HEADS * VDIM, D), (DIFF_HEADS * VDIM) ** -0.5, 0.125, ((0, 4),)),
        "proj_win": scatter_about(key_of[11], (WIN_HEADS * HEAD, D), (6 * (WIN_HEADS * HEAD) ** -0.5), 0.79296875, ((0, 4),)),
    }


EPS = 1e-06

def root_mean_square_rows(values, gain):
    return values * lax.rsqrt(lax.optimization_barrier(jnp.mean(values * values, axis=-1, keepdims=True)) + EPS) * gain

def reference(tokens, norm_gain, query_diff, key_diff, value_diff, lam, output_norm_gain, query_win, keyval_win, sink, proj_diff, proj_win):
    seq = tokens.shape[0]
    normed = root_mean_square_rows(tokens.astype(jnp.float32), norm_gain).astype(jnp.bfloat16)

    def project(weight):
        return jnp.dot(normed, weight, preferred_element_type=jnp.float32).astype(jnp.bfloat16)
    q_diff = project(query_diff).reshape(seq, DIFF_HEADS, 2, HEAD)
    k_diff = project(key_diff).reshape(seq, DIFF_HEADS, 2, HEAD)
    v_diff = project(value_diff).reshape(seq, DIFF_HEADS, VDIM)
    q_win = project(query_win).reshape(seq, WIN_HEADS, HEAD)
    kv_win = jnp.stack([project(keyval_win[g]) for g in range(KV_HEADS)], axis=1)
    scale = HEAD ** (-0.5)
    qblock = math.gcd(seq, 512)

    def diff_head(args):
        q_head, k_head, v_head, lambda_head = args

        def one_block(q_rows):
            output_list = []
            for m in range(2):
                scores = jnp.dot(q_rows[:, m], k_head[:, m].T, preferred_element_type=jnp.float32) * scale
                top = lax.optimization_barrier(jnp.max(scores, axis=-1, keepdims=True))
                expo = jnp.exp(scores - top)
                total = lax.optimization_barrier(jnp.sum(expo, axis=-1, keepdims=True))
                output_list.append(jnp.dot(expo.astype(jnp.bfloat16), v_head, preferred_element_type=jnp.float32) / total)
            difference_output = output_list[0] - lambda_head * output_list[1]
            return root_mean_square_rows(difference_output, output_norm_gain).astype(jnp.bfloat16)
        result = lax.map(one_block, q_head.reshape(seq // qblock, qblock, 2, HEAD))
        return result.reshape(seq, VDIM)
    differential_output = lax.map(diff_head, (jnp.transpose(q_diff, (1, 0, 2, 3)), jnp.transpose(k_diff, (1, 0, 2, 3)), jnp.transpose(v_diff, (1, 0, 2)), lam))
    differential_output = jnp.transpose(differential_output, (1, 0, 2)).reshape(seq, DIFF_HEADS * VDIM)
    group = WIN_HEADS // KV_HEADS
    nblocks = seq // WINDOW
    q_blocks = q_win.reshape(nblocks, WINDOW, KV_HEADS, group, HEAD).astype(jnp.float32)
    padded = jnp.pad(kv_win, ((WINDOW, WINDOW), (0, 0), (0, 0))).reshape(nblocks + 2, WINDOW, KV_HEADS, 2 * HEAD)
    band = jnp.concatenate([padded[:-2], padded[1:-1], padded[2:]], axis=1).astype(jnp.float32)
    scores = jnp.einsum('nqgrd,nkgd->ngrqk', q_blocks, band[..., :HEAD]) * scale
    q_index = jnp.arange(WINDOW, dtype=jnp.int32)
    k_index = jnp.arange(3 * WINDOW, dtype=jnp.int32)
    offset = k_index[None, :] - WINDOW - q_index[:, None]
    key_pos = jnp.arange(nblocks, dtype=jnp.int32)[:, None] * WINDOW - WINDOW + k_index[None, :]
    valid = (jnp.abs(offset) <= WINDOW)[None] & ((key_pos >= 0) & (key_pos < seq))[:, None, :]
    scores = jnp.where(valid[:, None, None], scores, -jnp.inf)
    sink_logit = sink.reshape(KV_HEADS, group)[:, :, None, None]
    top = jnp.maximum(lax.optimization_barrier(jnp.max(scores, axis=-1, keepdims=True)), sink_logit)
    expo = jnp.exp(scores - top)
    weights = expo / (lax.optimization_barrier(jnp.sum(expo, axis=-1, keepdims=True)) + jnp.exp(sink_logit - top))
    weights = weights.astype(jnp.bfloat16).astype(jnp.float32)
    y_win = jnp.einsum('ngrqk,nkgd->nqgrd', weights, band[..., HEAD:]).astype(jnp.bfloat16)
    y_win = y_win.reshape(seq, WIN_HEADS * HEAD)
    total = jnp.dot(differential_output, proj_diff, preferred_element_type=jnp.float32)
    total = total + jnp.dot(y_win, proj_win, preferred_element_type=jnp.float32)
    return total.astype(jnp.bfloat16)
```

```python
import math

import jax
import jax.numpy as jnp
from jax import lax
from jax.experimental import pallas as pl
from jax.experimental.pallas import tpu as pltpu
from jax.sharding import PartitionSpec as P

HEAD = 128
WIN_HEADS = 16
KV_HEADS = 4
WINDOW = 128
VDIM = 256
EPS = 1e-06
AXES = ("grp", "sp", "tp")

BF = jnp.bfloat16
F32 = jnp.float32


def padded_2(x, sides, width):
    for axis, dim in sides:
        devices, length = (lax.axis_size(axis), x.shape[dim])
        up = [(i, (i + 1) % devices) for i in range(devices - 1)]
        down = [(j, i) for i, j in up]
        last = lax.slice_in_dim(x, length - width, length, axis=dim)
        first = lax.slice_in_dim(x, 0, width, axis=dim)
        before = lax.ppermute(last, axis, up)
        after = lax.ppermute(first, axis, down)
        x = jnp.concatenate([before, x, after], axis=dim)
    return x


def root_mean_square_rows(values, gain):
    return values * lax.rsqrt(jnp.mean(values * values, axis=-1, keepdims=True) + EPS) * gain


def general_body(
    tokens,
    norm_gain,
    query_diff,
    key_diff,
    value_diff,
    lam,
    output_norm_gain,
    query_win,
    keyval_win,
    sink,
    proj_diff,
    proj_win,
):
    normed = root_mean_square_rows(tokens.astype(jnp.float32), norm_gain).astype(jnp.bfloat16)
    heads_diff = lam.shape[0]
    heads_win = sink.shape[0]
    group = WIN_HEADS // KV_HEADS
    kv_index = lax.axis_index("tp") * heads_win // group
    kv_local = lax.dynamic_index_in_dim(keyval_win, kv_index, 0, keepdims=False)
    pieces = [query_diff, key_diff, value_diff, query_win, kv_local]
    stacked = jnp.concatenate(pieces, axis=1)
    whole = lax.all_gather(stacked, "sp", axis=0, tiled=True)
    projected = jnp.dot(
        lax.all_gather(normed, "tp", axis=0, tiled=True), whole, preferred_element_type=jnp.float32
    )
    projected = projected.astype(jnp.bfloat16)
    output_list = []
    offset = 0
    for piece in pieces:
        output_list.append(projected[:, offset : offset + piece.shape[1]])
        offset = offset + piece.shape[1]
    q_diff, k_diff, v_diff, q_win, kv_win = output_list
    tok = projected.shape[0]
    scale = HEAD ** (-0.5)
    q_four = q_diff.reshape(tok, heads_diff, 2, HEAD)
    start_state = (
        jnp.full((heads_diff, 2, tok), -jnp.inf, jnp.float32),
        jnp.zeros((heads_diff, 2, tok), jnp.float32),
        jnp.zeros((heads_diff, 2, tok, VDIM), jnp.float32),
    )
    carry = start_state
    keys = lax.all_gather(k_diff, "sp", axis=0, tiled=True)
    values = lax.all_gather(v_diff, "sp", axis=0, tiled=True)
    rows = keys.shape[0]
    step = math.gcd(rows, 1024)
    key_blocks = keys.reshape(rows // step, step, heads_diff, 2, HEAD)
    value_blocks = values.reshape(rows // step, step, heads_diff, VDIM)

    def one(state, block):
        top, total, acc = state
        key_part, value_part = block
        scores = (
            jnp.einsum("qhmd,khmd->hmqk", q_four, key_part, preferred_element_type=jnp.float32)
            * scale
        )
        new_top = jnp.maximum(top, jnp.max(scores, axis=-1))
        expo = jnp.exp(scores - new_top[..., None])
        fade = jnp.exp(top - new_top)
        total = total * fade + jnp.sum(expo, axis=-1)
        acc = acc * fade[..., None] + jnp.einsum(
            "hmqk,khe->hmqe",
            expo.astype(jnp.bfloat16),
            value_part,
            preferred_element_type=jnp.float32,
        )
        return ((new_top, total, acc), None)

    carry, unused = lax.scan(one, carry, (key_blocks, value_blocks))
    top, total, acc = carry
    attention_maps = acc / total[..., None]
    difference_output = attention_maps[:, 0] - lam[:, None, None] * attention_maps[:, 1]
    differential_output = root_mean_square_rows(difference_output, output_norm_gain).astype(
        jnp.bfloat16
    )
    differential_output = jnp.transpose(differential_output, (1, 0, 2)).reshape(
        tok, heads_diff * VDIM
    )
    padded = padded_2(kv_win, (("sp", 0),), WINDOW)
    nblocks = tok // WINDOW
    blocks = padded.reshape(nblocks + 2, WINDOW, 2 * HEAD)
    band = jnp.concatenate([blocks[:-2], blocks[1:-1], blocks[2:]], axis=1)
    q_blocks = q_win.reshape(nblocks, WINDOW, heads_win, HEAD)
    scores = (
        jnp.einsum("nqhd,nkd->nhqk", q_blocks, band[..., :HEAD], preferred_element_type=jnp.float32)
        * scale
    )
    q_index = jnp.arange(WINDOW)
    k_index = jnp.arange(3 * WINDOW)
    relative = k_index[None, :] - WINDOW - q_index[:, None]
    first_key = lax.axis_index("sp") * tok - WINDOW
    key_pos = first_key + jnp.arange(nblocks)[:, None] * WINDOW + k_index[None, :]
    inside = (key_pos >= 0) & (key_pos < tok * lax.axis_size("sp"))
    valid = (jnp.abs(relative) <= WINDOW)[None] & inside[:, None, :]
    scores = jnp.where(valid[:, None], scores, -jnp.inf)
    sink_logit = sink[None, :, None, None]
    top_win = jnp.maximum(jnp.max(scores, axis=-1, keepdims=True), sink_logit)
    expo = jnp.exp(scores - top_win)
    weights = expo / (jnp.sum(expo, axis=-1, keepdims=True) + jnp.exp(sink_logit - top_win))
    y_win = jnp.einsum(
        "nhqk,nkd->nqhd",
        weights.astype(jnp.bfloat16),
        band[..., HEAD:],
        preferred_element_type=jnp.float32,
    ).astype(jnp.bfloat16)
    y_win = y_win.reshape(tok, heads_win * HEAD)
    summed = jnp.dot(differential_output, proj_diff, preferred_element_type=jnp.float32)
    return lax.psum_scatter(
        (summed + jnp.dot(y_win, proj_win, preferred_element_type=jnp.float32)).astype(
            jnp.bfloat16
        ),
        "tp",
        scatter_dimension=0,
        tiled=True,
    )


def attention_kernel(
    place, lam, sink, gain, q_ref, own_ref, oth_ref, out_ref, *, sp, nx, flip, scale
):
    slot = pl.program_id(0)
    s, x, c = place[0], place[1], place[2]
    rows = own_ref.shape[0]
    nt = (((1,), (1,)), ((), ()))
    maps = []
    for m in range(2):
        lanes = slice(m * HEAD, (m + 1) * HEAD)
        q = q_ref[:, lanes]
        sa = lax.dot_general(q, own_ref[:, lanes], nt, preferred_element_type=F32) * scale
        sb = lax.dot_general(q, oth_ref[:, lanes], nt, preferred_element_type=F32) * scale
        top = jnp.maximum(
            jnp.max(sa, axis=-1, keepdims=True), jnp.max(sb, axis=-1, keepdims=True)
        )
        ea = jnp.exp(sa - top)
        eb = jnp.exp(sb - top)
        total = jnp.sum(ea, axis=-1, keepdims=True) + jnp.sum(eb, axis=-1, keepdims=True)
        acc = jnp.dot(ea.astype(BF), own_ref[:, 256:512], preferred_element_type=F32)
        acc = acc + jnp.dot(eb.astype(BF), oth_ref[:, 256:512], preferred_element_type=F32)
        maps.append(acc / total)
    d = maps[0] - lam[0] * maps[1]
    y = d * lax.rsqrt(jnp.mean(d * d, axis=-1, keepdims=True) + EPS) * gain[...]
    out_ref[:, 0:VDIM] = y.astype(BF)

    def row_of(i):
        return ((i % nx) ^ x) * (rows // nx) + ((i // nx) ^ s) * WINDOW

    last = rows // WINDOW - 1
    i = (slot ^ s) * nx + (x ^ flip)
    before = i - 1 + c
    after = i + c
    r_own = pl.multiple_of(row_of(i), WINDOW)
    r_bef = pl.multiple_of(row_of(jnp.maximum(before, 0)), WINDOW)
    r_aft = pl.multiple_of(row_of(jnp.minimum(after, last)), WINDOW)
    kw = slice(512, 512 + HEAD)
    vw = slice(512 + HEAD, 512 + 2 * HEAD)
    k0 = oth_ref[pl.ds(r_bef, WINDOW), kw]
    k1 = own_ref[pl.ds(r_own, WINDOW), kw]
    k2 = oth_ref[pl.ds(r_aft, WINDOW), kw]
    v0 = oth_ref[pl.ds(r_bef, WINDOW), vw]
    v1 = own_ref[pl.ds(r_own, WINDOW), vw]
    v2 = oth_ref[pl.ds(r_aft, WINDOW), vw]
    q_at = lax.broadcasted_iota(jnp.int32, (WINDOW, WINDOW), 0)
    k_at = lax.broadcasted_iota(jnp.int32, (WINDOW, WINDOW), 1)
    ok0 = (k_at >= q_at) & (before >= 0)
    ok2 = (k_at <= q_at) & (after <= last)
    for h in range(2):
        q = q_ref[:, 256 + h * HEAD : 256 + (h + 1) * HEAD]
        z0 = lax.dot_general(q, k0, nt, preferred_element_type=F32) * scale
        z1 = lax.dot_general(q, k1, nt, preferred_element_type=F32) * scale
        z2 = lax.dot_general(q, k2, nt, preferred_element_type=F32) * scale
        z0 = jnp.where(ok0, z0, -jnp.inf)
        z2 = jnp.where(ok2, z2, -jnp.inf)
        top = jnp.max(jnp.maximum(jnp.maximum(z0, z1), z2), axis=-1, keepdims=True)
        top = jnp.maximum(top, sink[h])
        e0, e1, e2 = jnp.exp(z0 - top), jnp.exp(z1 - top), jnp.exp(z2 - top)
        total = jnp.sum(e0 + e1 + e2, axis=-1, keepdims=True) + jnp.exp(sink[h] - top)
        w = 1.0 / total
        acc = jnp.dot((e0 * w).astype(BF), v0, preferred_element_type=F32)
        acc = acc + jnp.dot((e1 * w).astype(BF), v1, preferred_element_type=F32)
        acc = acc + jnp.dot((e2 * w).astype(BF), v2, preferred_element_type=F32)
        out_ref[:, VDIM + h * HEAD : VDIM + (h + 1) * HEAD] = acc.astype(BF)


def attention(place, lam, sink, gain, q, own, oth, sp, nx, flip):
    rows = own.shape[0]
    smem = pl.BlockSpec(memory_space=pltpu.SMEM)
    whole = pl.BlockSpec(own.shape, lambda i: (0, 0))

    def kernel(*refs):
        attention_kernel(*refs, sp=sp, nx=nx, flip=flip, scale=HEAD**-0.5)

    return pl.pallas_call(
        kernel,
        grid=(sp,),
        in_specs=[
            smem,
            smem,
            smem,
            pl.BlockSpec((1, VDIM), lambda i: (0, 0)),
            pl.BlockSpec((WINDOW, 512), lambda i: (i, 0)),
            whole,
            whole,
        ],
        out_specs=pl.BlockSpec((WINDOW, 512), lambda i: (i, 0)),
        out_shape=jax.ShapeDtypeStruct((sp * WINDOW, 512), BF),
        compiler_params=pltpu.CompilerParams(dimension_semantics=("arbitrary",)),
        name="attend",
    )(place, lam, sink, gain, q, own, oth)


def chip_body(
    tokens,
    norm_gain,
    query_diff,
    key_diff,
    value_diff,
    lam,
    output_norm_gain,
    query_win,
    keyval_win,
    sink,
    proj_diff,
    proj_win,
):
    ng, sp, tp = (lax.axis_size(a) for a in AXES)
    nx = tp // 2
    g, s, t = (lax.axis_index(a) for a in AXES)
    x, c = t // 2, t % 2

    def send(value, target, only=None):
        pairs = []
        for i in range(ng * sp * tp):
            at = (i // (sp * tp), i // tp % sp, i % tp // 2, i % 2)
            if only is None or only(*at):
                a, b, d, e = target(*at)
                pairs.append((i, ((a * sp + b) * nx + d) * 2 + e))
        return lax.ppermute(value, AXES, pairs)

    def over_core(v):
        return send(v, lambda a, b, d, e: (a, b, d, e ^ 1))

    def over_x(v):
        return send(v, lambda a, b, d, e: (a, b, d ^ 1, e))

    def over_y(v):
        return send(v, lambda a, b, d, e: (a ^ 1, b, d, e))

    def over_z(v, k):
        return send(v, lambda a, b, d, e: (a, b ^ k, d, e))

    def mids(v, k):
        return send(v, lambda a, b, d, e: (a, b ^ k, d, e), lambda a, b, d, e: b in (1, 2))

    mid = (s == 1) | (s == 2)
    normed = root_mean_square_rows(tokens.astype(F32), norm_gain).astype(BF)
    one = over_z(normed, 1)
    near = mids(normed, 3)
    far = mids(near, 1)
    cross = mids(one, 3)
    slot2 = jnp.where(mid, cross, far)
    last = mids(cross, 1)
    slot3 = jnp.where(mid, near, last)
    mine = [normed, one, slot2, slot3]
    theirs = [over_x(v) for v in mine]
    acts = jnp.concatenate(mine + theirs, axis=0)

    rows_w = query_diff.shape[0]
    quarter = rows_w // 4

    def pack(lo, size, head):
        parts = []
        for w in (query_diff, query_win, key_diff, value_diff):
            parts.append(lax.dynamic_slice(w, (lo, head * VDIM), (size, VDIM)))
        return jnp.concatenate(parts, axis=1)

    def kv_pack(lo, size, h):
        kv = lax.dynamic_slice(
            keyval_win, (nx * x + h // 2, lo, 0), (1, size, 2 * HEAD)
        )
        return kv[0]

    mine_lo = (g * 2 + c) * quarter
    give_lo = (g * 2 + 1 - c) * quarter
    give = jnp.stack([pack(give_lo, quarter, 0), pack(give_lo, quarter, 1)])
    keep = jnp.stack([pack(mine_lo, quarter, 0), pack(mine_lo, quarter, 1)])
    both = jnp.concatenate([keep, over_core(give)], axis=0)
    weights = jnp.zeros((sp * rows_w, 5 * VDIM), BF)
    local = pack(0, rows_w, s % 2)
    moved = send(
        local, lambda a, b, d, e: (a, b, d, e ^ 1), lambda a, b, d, e: e == b // 2
    )
    own = jnp.where(c == s // 2, local, moved)
    own = jnp.concatenate([own, kv_pack(0, rows_w, s)], axis=1)
    weights = lax.dynamic_update_slice(weights, own, (s * rows_w, 0))
    for k in range(1, sp):
        h = s ^ k
        pick = lax.dynamic_index_in_dim(both, ((h // 2) ^ c) * 2 + h % 2, 0, keepdims=False)
        part = jnp.concatenate([pick, kv_pack(mine_lo, quarter, h)], axis=1)
        got = over_z(part, k)
        got_y = over_y(got)
        pair = over_core(jnp.stack([got, got_y]))
        base = (s ^ k) * rows_w
        for piece, gg, cc in (
            (got, g, c),
            (got_y, 1 - g, c),
            (pair[0], g, 1 - c),
            (pair[1], 1 - g, 1 - c),
        ):
            weights = lax.dynamic_update_slice(
                weights, piece, (base + (gg * 2 + cc) * quarter, 0)
            )

    projected = jnp.dot(acts, weights, preferred_element_type=F32).astype(BF)
    queries = projected[:, : 2 * VDIM]
    kv_own = projected[:, 2 * VDIM :]
    kv_oth = over_core(kv_own)

    lam_both = jnp.concatenate([lam, over_core(lam)])
    sink_both = jnp.concatenate([sink, over_core(sink)])
    at = ((s // 2) ^ c) * 2 + s % 2
    lam_one = lax.dynamic_slice(lam_both, (at,), (1,))
    sink_two = lax.dynamic_slice(sink_both, (at * 2,), (2,))
    place = jnp.stack([s, x, c]).astype(jnp.int32)
    gain = output_norm_gain.reshape(1, VDIM)
    half = queries.shape[0] // 2
    pd_oth = over_core(proj_diff)
    pw_oth = over_core(proj_win)

    def mix(y):
        y = y.reshape(sp, WINDOW, 2 * VDIM)
        got = [y[0]] + [over_z(y[k], k) for k in range(1, sp)]
        stacked = jnp.stack(got)

        def head(h):
            return lax.dynamic_index_in_dim(stacked, h ^ s, 0, keepdims=False)

        total = jnp.zeros((WINDOW, proj_diff.shape[1]), F32)
        for core, pd, pw in ((c, proj_diff, proj_win), (1 - c, pd_oth, pw_oth)):
            h0, h1 = head(core * 2), head(core * 2 + 1)
            yd = jnp.concatenate([h0[:, :VDIM], h1[:, :VDIM]], axis=1)
            yw = jnp.concatenate([h0[:, VDIM:], h1[:, VDIM:]], axis=1)
            total = total + jnp.dot(yd, pd, preferred_element_type=F32)
            total = total + jnp.dot(yw, pw, preferred_element_type=F32)
        return total

    y_far = attention(place, lam_one, sink_two, gain, queries[half:], kv_own, kv_oth, sp, nx, 1)
    y_near = attention(place, lam_one, sink_two, gain, queries[:half], kv_own, kv_oth, sp, nx, 0)
    moved_out = over_x(mix(y_far).astype(BF))
    return (mix(y_near) + moved_out.astype(F32)).astype(BF)


def solution(mesh):
    placed = (
        P(("grp", "sp", "tp"), None),
        P(),
        P("sp", "tp"),
        P("sp", "tp"),
        P("sp", "tp"),
        P("tp"),
        P(),
        P("sp", "tp"),
        P(None, "sp", None),
        P("tp"),
        P("tp", None),
        P("tp", None),
    )
    sizes = dict(mesh.shape)

    def body(*args):
        tokens, lam, sink = args[0], args[5], args[9]
        fits = (
            sizes["grp"] == 2
            and sizes["sp"] == 4
            and sizes["tp"] == 4
            and tokens.shape[0] == WINDOW
            and lam.shape[0] == 2
            and sink.shape[0] == 4
        )
        return (chip_body if fits else general_body)(*args)

    return jax.shard_map(
        body, mesh=mesh, in_specs=placed, out_specs=P(("grp", "sp", "tp"), None), check_vma=False
    )
```

```python
import math

import jax
import jax.numpy as jnp
from jax import lax
from jax.experimental import pallas as pl
from jax.experimental.pallas import tpu as pltpu
from jax.sharding import PartitionSpec as P


HEAD = 128
WIN_HEADS = 16
KV_HEADS = 4
WINDOW = 128
VDIM = 256
EPS = 1e-06
AXES = ("grp", "sp", "tp")

BF = jnp.bfloat16
F32 = jnp.float32


def padded_2(x, sides, width):
    for axis, dim in sides:
        devices, length = (lax.axis_size(axis), x.shape[dim])
        up = [(i, (i + 1) % devices) for i in range(devices - 1)]
        down = [(j, i) for i, j in up]
        last = lax.slice_in_dim(x, length - width, length, axis=dim)
        first = lax.slice_in_dim(x, 0, width, axis=dim)
        before = lax.ppermute(last, axis, up)
        after = lax.ppermute(first, axis, down)
        x = jnp.concatenate([before, x, after], axis=dim)
    return x


def root_mean_square_rows(values, gain):
    return values * lax.rsqrt(jnp.mean(values * values, axis=-1, keepdims=True) + EPS) * gain


def general_body(
    tokens,
    norm_gain,
    query_diff,
    key_diff,
    value_diff,
    lam,
    output_norm_gain,
    query_win,
    keyval_win,
    sink,
    proj_diff,
    proj_win,
):
    normed = root_mean_square_rows(tokens.astype(jnp.float32), norm_gain).astype(jnp.bfloat16)
    heads_diff = lam.shape[0]
    heads_win = sink.shape[0]
    group = WIN_HEADS // KV_HEADS
    kv_index = lax.axis_index("tp") * heads_win // group
    kv_local = lax.dynamic_index_in_dim(keyval_win, kv_index, 0, keepdims=False)
    pieces = [query_diff, key_diff, value_diff, query_win, kv_local]
    stacked = jnp.concatenate(pieces, axis=1)
    whole = lax.all_gather(stacked, "sp", axis=0, tiled=True)
    projected = jnp.dot(
        lax.all_gather(normed, "tp", axis=0, tiled=True), whole, preferred_element_type=jnp.float32
    )
    projected = projected.astype(jnp.bfloat16)
    output_list = []
    offset = 0
    for piece in pieces:
        output_list.append(projected[:, offset : offset + piece.shape[1]])
        offset = offset + piece.shape[1]
    q_diff, k_diff, v_diff, q_win, kv_win = output_list
    tok = projected.shape[0]
    scale = HEAD ** (-0.5)
    q_four = q_diff.reshape(tok, heads_diff, 2, HEAD)
    start_state = (
        jnp.full((heads_diff, 2, tok), -jnp.inf, jnp.float32),
        jnp.zeros((heads_diff, 2, tok), jnp.float32),
        jnp.zeros((heads_diff, 2, tok, VDIM), jnp.float32),
    )
    carry = start_state
    keys = lax.all_gather(k_diff, "sp", axis=0, tiled=True)
    values = lax.all_gather(v_diff, "sp", axis=0, tiled=True)
    rows = keys.shape[0]
    step = math.gcd(rows, 1024)
    key_blocks = keys.reshape(rows // step, step, heads_diff, 2, HEAD)
    value_blocks = values.reshape(rows // step, step, heads_diff, VDIM)

    def one(state, block):
        top, total, acc = state
        key_part, value_part = block
        scores = (
            jnp.einsum("qhmd,khmd->hmqk", q_four, key_part, preferred_element_type=jnp.float32)
            * scale
        )
        new_top = jnp.maximum(top, jnp.max(scores, axis=-1))
        expo = jnp.exp(scores - new_top[..., None])
        fade = jnp.exp(top - new_top)
        total = total * fade + jnp.sum(expo, axis=-1)
        acc = acc * fade[..., None] + jnp.einsum(
            "hmqk,khe->hmqe",
            expo.astype(jnp.bfloat16),
            value_part,
            preferred_element_type=jnp.float32,
        )
        return ((new_top, total, acc), None)

    carry, _ = lax.scan(one, carry, (key_blocks, value_blocks))
    _, total, acc = carry
    attention_maps = acc / total[..., None]
    difference_output = attention_maps[:, 0] - lam[:, None, None] * attention_maps[:, 1]
    differential_output = root_mean_square_rows(difference_output, output_norm_gain).astype(
        jnp.bfloat16
    )
    differential_output = jnp.transpose(differential_output, (1, 0, 2)).reshape(
        tok, heads_diff * VDIM
    )
    padded = padded_2(kv_win, (("sp", 0),), WINDOW)
    nblocks = tok // WINDOW
    blocks = padded.reshape(nblocks + 2, WINDOW, 2 * HEAD)
    band = jnp.concatenate([blocks[:-2], blocks[1:-1], blocks[2:]], axis=1)
    q_blocks = q_win.reshape(nblocks, WINDOW, heads_win, HEAD)
    scores = (
        jnp.einsum("nqhd,nkd->nhqk", q_blocks, band[..., :HEAD], preferred_element_type=jnp.float32)
        * scale
    )
    q_index = jnp.arange(WINDOW)
    k_index = jnp.arange(3 * WINDOW)
    relative = k_index[None, :] - WINDOW - q_index[:, None]
    first_key = lax.axis_index("sp") * tok - WINDOW
    key_pos = first_key + jnp.arange(nblocks)[:, None] * WINDOW + k_index[None, :]
    inside = (key_pos >= 0) & (key_pos < tok * lax.axis_size("sp"))
    valid = (jnp.abs(relative) <= WINDOW)[None] & inside[:, None, :]
    scores = jnp.where(valid[:, None], scores, -jnp.inf)
    sink_logit = sink[None, :, None, None]
    top_win = jnp.maximum(jnp.max(scores, axis=-1, keepdims=True), sink_logit)
    expo = jnp.exp(scores - top_win)
    weights = expo / (jnp.sum(expo, axis=-1, keepdims=True) + jnp.exp(sink_logit - top_win))
    y_win = jnp.einsum(
        "nhqk,nkd->nqhd",
        weights.astype(jnp.bfloat16),
        band[..., HEAD:],
        preferred_element_type=jnp.float32,
    ).astype(jnp.bfloat16)
    y_win = y_win.reshape(tok, heads_win * HEAD)
    summed = jnp.dot(differential_output, proj_diff, preferred_element_type=jnp.float32)
    return lax.psum_scatter(
        (summed + jnp.dot(y_win, proj_win, preferred_element_type=jnp.float32)).astype(
            jnp.bfloat16
        ),
        "tp",
        scatter_dimension=0,
        tiled=True,
    )


def attention_kernel(
    place, lam, sink, gain, q_ref, own_ref, oth_ref, out_ref, *, nx, flip, scale, blocks
):
    step = pl.program_id(0)
    s, x, c = place[0], place[1], place[2]
    rows = own_ref.shape[0]
    nt = (((1,), (1,)), ((), ()))
    maps = []
    for m in range(2):
        lanes = slice(m * HEAD, (m + 1) * HEAD)
        q = q_ref[:, lanes]
        sa = lax.dot_general(q, own_ref[:, lanes], nt, preferred_element_type=F32) * scale
        sb = lax.dot_general(q, oth_ref[:, lanes], nt, preferred_element_type=F32) * scale
        top = jnp.maximum(
            jnp.max(sa, axis=-1, keepdims=True), jnp.max(sb, axis=-1, keepdims=True)
        )
        ea = jnp.exp(sa - top)
        eb = jnp.exp(sb - top)
        total = jnp.sum(ea, axis=-1, keepdims=True) + jnp.sum(eb, axis=-1, keepdims=True)
        acc = jnp.dot(ea.astype(BF), own_ref[:, 256:512], preferred_element_type=F32)
        acc = acc + jnp.dot(eb.astype(BF), oth_ref[:, 256:512], preferred_element_type=F32)
        maps.append(acc / total)
    d = maps[0] - lam[0] * maps[1]
    y = d * lax.rsqrt(jnp.mean(d * d, axis=-1, keepdims=True) + EPS) * gain[...]
    out_ref[:, 0:VDIM] = y.astype(BF)

    def row_of(i):
        return ((i % nx) ^ x) * (rows // nx) + ((i // nx) ^ s) * WINDOW

    last = rows // WINDOW - 1
    kw = slice(512, 512 + HEAD)
    vw = slice(512 + HEAD, 512 + 2 * HEAD)
    q_at = lax.broadcasted_iota(jnp.int32, (WINDOW, WINDOW), 0)
    k_at = lax.broadcasted_iota(jnp.int32, (WINDOW, WINDOW), 1)
    for block in range(blocks):
        slot = step * blocks + block
        here = slice(block * WINDOW, (block + 1) * WINDOW)
        i = (slot ^ s) * nx + (x ^ flip)
        before = i - 1 + c
        after = i + c
        r_own = pl.multiple_of(row_of(i), WINDOW)
        r_bef = pl.multiple_of(row_of(jnp.maximum(before, 0)), WINDOW)
        r_aft = pl.multiple_of(row_of(jnp.minimum(after, last)), WINDOW)
        k0 = oth_ref[pl.ds(r_bef, WINDOW), kw]
        k1 = own_ref[pl.ds(r_own, WINDOW), kw]
        k2 = oth_ref[pl.ds(r_aft, WINDOW), kw]
        v0 = oth_ref[pl.ds(r_bef, WINDOW), vw]
        v1 = own_ref[pl.ds(r_own, WINDOW), vw]
        v2 = oth_ref[pl.ds(r_aft, WINDOW), vw]
        ok0 = (k_at >= q_at) & (before >= 0)
        ok2 = (k_at <= q_at) & (after <= last)
        for h in range(2):
            q = q_ref[here, 256 + h * HEAD : 256 + (h + 1) * HEAD]
            z0 = lax.dot_general(q, k0, nt, preferred_element_type=F32) * scale
            z1 = lax.dot_general(q, k1, nt, preferred_element_type=F32) * scale
            z2 = lax.dot_general(q, k2, nt, preferred_element_type=F32) * scale
            z0 = jnp.where(ok0, z0, -jnp.inf)
            z2 = jnp.where(ok2, z2, -jnp.inf)
            top = jnp.max(jnp.maximum(jnp.maximum(z0, z1), z2), axis=-1, keepdims=True)
            top = jnp.maximum(top, sink[h])
            e0, e1, e2 = jnp.exp(z0 - top), jnp.exp(z1 - top), jnp.exp(z2 - top)
            total = jnp.sum(e0 + e1 + e2, axis=-1, keepdims=True) + jnp.exp(sink[h] - top)
            w = 1.0 / total
            acc = jnp.dot((e0 * w).astype(BF), v0, preferred_element_type=F32)
            acc = acc + jnp.dot((e1 * w).astype(BF), v1, preferred_element_type=F32)
            acc = acc + jnp.dot((e2 * w).astype(BF), v2, preferred_element_type=F32)
            out_ref[here, VDIM + h * HEAD : VDIM + (h + 1) * HEAD] = acc.astype(BF)


def attention(place, lam, sink, gain, q, own, oth, sp, nx, flip, blocks=2):
    rows = own.shape[0]
    smem = pl.BlockSpec(memory_space=pltpu.SMEM)
    whole = pl.BlockSpec(own.shape, lambda i: (0, 0))
    steps = sp // blocks
    size = blocks * WINDOW

    def kernel(*refs):
        attention_kernel(*refs, nx=nx, flip=flip, scale=HEAD**-0.5, blocks=blocks)

    return pl.pallas_call(
        kernel,
        grid=(steps,),
        in_specs=[
            smem,
            smem,
            smem,
            pl.BlockSpec((1, VDIM), lambda i: (0, 0)),
            pl.BlockSpec((size, 512), lambda i: (flip * steps + i, 0)),
            whole,
            whole,
        ],
        out_specs=pl.BlockSpec((size, 512), lambda i: (i, 0)),
        out_shape=jax.ShapeDtypeStruct((sp * WINDOW, 512), BF),
        compiler_params=pltpu.CompilerParams(dimension_semantics=("arbitrary",)),
        cost_estimate=pl.CostEstimate(
            flops=4 * sp * WINDOW * rows * 2 * 384, bytes_accessed=4 * 2**20, transcendentals=0
        ),
        name="attend",
    )(place, lam, sink, gain, q, own, oth)


def project(where, acts, pieces, acc, first, count, kind):
    rows = acts.shape[0]
    size = pieces[0].shape[0]
    wide = size * len(pieces)

    def kernel(where_ref, acts_ref, *refs):
        weights, rest = refs[: len(pieces)], refs[len(pieces) :]
        total = rest[0][...] if acc is not None else None
        for j, w in enumerate(weights):
            if len(pieces) == 1:
                a = acts_ref[...]
            else:
                a = acts_ref[:, pl.ds(pl.multiple_of(where_ref[1 + j], size), size)]
            part = jnp.dot(a, w[...], preferred_element_type=F32)
            total = part if total is None else total + part
        rest[-1][...] = total.astype(kind)

    in_specs = [pl.BlockSpec((rows, wide), lambda n, at: (0, at[0]))]
    in_specs += [pl.BlockSpec((size, 256), lambda n, at: (0, n + first)) for _ in pieces]
    operands = [acts, *pieces]
    if acc is not None:
        in_specs.append(pl.BlockSpec((rows, 256), lambda n, at: (0, n + first)))
        operands.append(acc)
    return pl.pallas_call(
        kernel,
        grid_spec=pltpu.PrefetchScalarGridSpec(
            num_scalar_prefetch=1,
            grid=(count,),
            in_specs=in_specs,
            out_specs=pl.BlockSpec((rows, 256), lambda n, at: (0, n)),
        ),
        out_shape=jax.ShapeDtypeStruct((rows, count * 256), kind),
        compiler_params=pltpu.CompilerParams(dimension_semantics=("arbitrary",)),
        cost_estimate=pl.CostEstimate(
            flops=2 * rows * wide * 256 * count,
            bytes_accessed=rows * 256 * count * 8,
            transcendentals=0,
        ),
        name="project",
    )(where, *operands)


def output_projection(place, heads, weights, extra):
    sp = len(heads)
    width = weights[0].shape[1]
    tile = 512

    def kernel(place_ref, *refs):
        ys, ws, rest = refs[:sp], refs[sp : sp + 4], refs[sp + 4 :]
        ordered, out = rest[-1], rest[-2]
        s, c = place_ref[0], place_ref[2]

        @pl.when(pl.program_id(0) == 0)
        def _():
            for k, y in enumerate(ys):
                ordered[(s ^ k) ^ (2 * c)] = y[...]

        total = rest[0][...].astype(F32) if extra is not None else None
        for j, w in enumerate(ws):
            lanes = slice((j % 2) * VDIM, (j % 2 + 1) * VDIM)
            for local in range(2):
                part = jnp.dot(
                    ordered[(j // 2) * 2 + local, :, lanes],
                    w[local * VDIM : (local + 1) * VDIM],
                    preferred_element_type=F32,
                )
                total = part if total is None else total + part
        out[...] = total.astype(out.dtype)

    whole = pl.BlockSpec((WINDOW, 2 * VDIM), lambda n: (0, 0))
    column = pl.BlockSpec((WINDOW, tile), lambda n: (0, n))
    in_specs = [pl.BlockSpec(memory_space=pltpu.SMEM)] + [whole] * sp
    in_specs += [pl.BlockSpec((2 * VDIM, tile), lambda n: (0, n))] * 4
    operands = [place, *heads, *weights]
    if extra is not None:
        in_specs.append(column)
        operands.append(extra)
    return pl.pallas_call(
        kernel,
        grid=(width // tile,),
        in_specs=in_specs,
        out_specs=column,
        out_shape=jax.ShapeDtypeStruct((WINDOW, width), BF),
        scratch_shapes=[pltpu.VMEM((sp, WINDOW, 2 * VDIM), BF)],
        compiler_params=pltpu.CompilerParams(dimension_semantics=("arbitrary",)),
        cost_estimate=pl.CostEstimate(
            flops=2 * WINDOW * 2048 * width, bytes_accessed=2048 * width * 2, transcendentals=0
        ),
        name="output",
    )(*operands)


def chip_body(
    tokens,
    norm_gain,
    query_diff,
    key_diff,
    value_diff,
    lam,
    output_norm_gain,
    query_win,
    keyval_win,
    sink,
    proj_diff,
    proj_win,
):
    ng, sp, tp = (lax.axis_size(a) for a in AXES)
    nx = tp // 2
    g, s, t = (lax.axis_index(a) for a in AXES)
    x, c = t // 2, t % 2

    def send(value, target, only=None):
        pairs = []
        for i in range(ng * sp * tp):
            at = (i // (sp * tp), i // tp % sp, i % tp // 2, i % 2)
            if only is None or only(*at):
                a, b, d, e = target(*at)
                pairs.append((i, ((a * sp + b) * nx + d) * 2 + e))
        return lax.ppermute(value, AXES, pairs)

    def over_core(v):
        return send(v, lambda a, b, d, e: (a, b, d, e ^ 1))

    def over_x(v):
        return send(v, lambda a, b, d, e: (a, b, d ^ 1, e))

    def over_y(v):
        return send(v, lambda a, b, d, e: (a ^ 1, b, d, e))

    def over_z(v, k):
        return send(v, lambda a, b, d, e: (a, b ^ k, d, e))

    def mids(v, k):
        return send(v, lambda a, b, d, e: (a, b ^ k, d, e), lambda a, b, d, e: b in (1, 2))

    mid = (s == 1) | (s == 2)
    normed = root_mean_square_rows(tokens.astype(F32), norm_gain).astype(BF)
    one = over_z(normed, 1)
    near = mids(normed, 3)
    tx0 = over_x(normed)
    far = mids(near, 1)
    cross = mids(one, 3)
    tx1 = over_x(one)
    last = mids(cross, 1)
    slot2 = jnp.where(mid, cross, far)
    tx2 = over_x(slot2)
    slot3 = jnp.where(mid, near, last)
    tx3 = over_x(slot3)
    acts = jnp.concatenate([normed, one, slot2, slot3, tx0, tx1, tx2, tx3], axis=0)

    rows_w = query_diff.shape[0]
    quarter = rows_w // 4

    def pack(lo, size, head):
        parts = []
        for w in (key_diff, value_diff, query_diff, query_win):
            parts.append(lax.dynamic_slice(w, (lo, head * VDIM), (size, VDIM)))
        return jnp.concatenate(parts, axis=1)

    def kv_pack(lo, size, h):
        kv = lax.dynamic_slice(keyval_win, (nx * x + h // 2, lo, 0), (1, size, 2 * HEAD))
        return kv[0]

    def with_kv(four, kv):
        return jnp.concatenate([four[:, : 2 * VDIM], kv, four[:, 2 * VDIM :]], axis=1)

    mine_lo = (g * 2 + c) * quarter
    give_lo = (g * 2 + 1 - c) * quarter
    give = jnp.stack([pack(give_lo, quarter, 0), pack(give_lo, quarter, 1)])
    keep = jnp.stack([pack(mine_lo, quarter, 0), pack(mine_lo, quarter, 1)])
    both = jnp.concatenate([keep, over_core(give)], axis=0)
    local = pack(0, rows_w, s % 2)
    moved = send(local, lambda a, b, d, e: (a, b, d, e ^ 1), lambda a, b, d, e: e == b // 2)
    own = with_kv(jnp.where(c == s // 2, local, moved), kv_pack(0, rows_w, s))

    def chunk(k):
        h = s ^ k
        pick = lax.dynamic_index_in_dim(both, ((h // 2) ^ c) * 2 + h % 2, 0, keepdims=False)
        part = with_kv(pick, kv_pack(mine_lo, quarter, h))
        got = over_z(part, k)
        got_c = over_core(got)
        got_y = over_y(got)
        got_yc = over_core(got_y)
        return [got, got_y, got_c, got_yc]

    def offset(gg, cc):
        return (gg * 2 + cc) * quarter

    def spot(k):
        return jnp.stack(
            [s ^ k, offset(g, c), offset(1 - g, c), offset(g, 1 - c), offset(1 - g, 1 - c)]
        ).astype(jnp.int32)

    chunks = {k: chunk(k) for k in (3, 2, 1)}
    acc = project(spot(0), acts, [own], None, 0, 5, F32)
    acc = project(spot(3), acts, chunks[3], acc, 0, 5, F32)
    acc = project(spot(2), acts, chunks[2], acc, 0, 5, F32)
    kv_own = project(spot(1), acts, chunks[1], acc, 0, 3, BF)
    kv_oth = over_core(kv_own)
    queries = project(spot(1), acts, chunks[1], acc, 3, 2, BF)

    lam_both = jnp.concatenate([lam, over_core(lam)])
    sink_both = jnp.concatenate([sink, over_core(sink)])
    at = ((s // 2) ^ c) * 2 + s % 2
    lam_one = lax.dynamic_slice(lam_both, (at,), (1,))
    sink_two = lax.dynamic_slice(sink_both, (at * 2,), (2,))
    place = jnp.stack([s, x, c]).astype(jnp.int32)
    gain = output_norm_gain.reshape(1, VDIM)
    weights = [proj_diff, proj_win, over_core(proj_diff), over_core(proj_win)]

    def spread(y):
        y = y.reshape(sp, WINDOW, 2 * VDIM)
        return [y[0]] + [over_z(y[k], k) for k in range(1, sp)]

    y_far = attention(place, lam_one, sink_two, gain, queries, kv_own, kv_oth, sp, nx, 1)
    y_near = attention(place, lam_one, sink_two, gain, queries, kv_own, kv_oth, sp, nx, 0)
    part = output_projection(place, spread(y_far), weights, None)
    received = over_x(part)
    return output_projection(place, spread(y_near), weights, received)


def solution(mesh):
    placed = (
        P(("grp", "sp", "tp"), None),
        P(),
        P("sp", "tp"),
        P("sp", "tp"),
        P("sp", "tp"),
        P("tp"),
        P(),
        P("sp", "tp"),
        P(None, "sp", None),
        P("tp"),
        P("tp", None),
        P("tp", None),
    )
    sizes = dict(mesh.shape)

    def body(*args):
        tokens, lam, sink = args[0], args[5], args[9]
        fits = (
            sizes["grp"] == 2
            and sizes["sp"] == 4
            and sizes["tp"] == 4
            and tokens.shape[0] == WINDOW
            and lam.shape[0] == 2
            and sink.shape[0] == 4
        )
        return (chip_body if fits else general_body)(*args)

    return jax.shard_map(
        body, mesh=mesh, in_specs=placed, out_specs=P(("grp", "sp", "tp"), None), check_vma=False
    )
```

```python
import math

import jax
import jax.numpy as jnp
from jax import lax
from jax.experimental import pallas as pl
from jax.experimental.pallas import tpu as pltpu
from jax.sharding import PartitionSpec as P


HEAD = 128
WIN_HEADS = 16
KV_HEADS = 4
WINDOW = 128
VDIM = 256
EPS = 1e-06
LOG2E = math.log2(math.e)
AXES = ("grp", "sp", "tp")

OUT_TILE = 1024
BF = jnp.bfloat16
F32 = jnp.float32


def padded_2(x, sides, width):
    for axis, dim in sides:
        devices, length = (lax.axis_size(axis), x.shape[dim])
        up = [(i, (i + 1) % devices) for i in range(devices - 1)]
        down = [(j, i) for i, j in up]
        last = lax.slice_in_dim(x, length - width, length, axis=dim)
        first = lax.slice_in_dim(x, 0, width, axis=dim)
        before = lax.ppermute(last, axis, up)
        after = lax.ppermute(first, axis, down)
        x = jnp.concatenate([before, x, after], axis=dim)
    return x


def root_mean_square_rows(values, gain):
    return values * lax.rsqrt(jnp.mean(values * values, axis=-1, keepdims=True) + EPS) * gain


def general_body(
    tokens,
    norm_gain,
    query_diff,
    key_diff,
    value_diff,
    lam,
    output_norm_gain,
    query_win,
    keyval_win,
    sink,
    proj_diff,
    proj_win,
):
    normed = root_mean_square_rows(tokens.astype(jnp.float32), norm_gain).astype(jnp.bfloat16)
    heads_diff = lam.shape[0]
    heads_win = sink.shape[0]
    group = WIN_HEADS // KV_HEADS
    kv_index = lax.axis_index("tp") * heads_win // group
    kv_local = lax.dynamic_index_in_dim(keyval_win, kv_index, 0, keepdims=False)
    pieces = [query_diff, key_diff, value_diff, query_win, kv_local]
    stacked = jnp.concatenate(pieces, axis=1)
    whole = lax.all_gather(stacked, "sp", axis=0, tiled=True)
    projected = jnp.dot(
        lax.all_gather(normed, "tp", axis=0, tiled=True), whole, preferred_element_type=jnp.float32
    )
    projected = projected.astype(jnp.bfloat16)
    output_list = []
    offset = 0
    for piece in pieces:
        output_list.append(projected[:, offset : offset + piece.shape[1]])
        offset = offset + piece.shape[1]
    q_diff, k_diff, v_diff, q_win, kv_win = output_list
    tok = projected.shape[0]
    scale = HEAD ** (-0.5)
    q_four = q_diff.reshape(tok, heads_diff, 2, HEAD)
    start_state = (
        jnp.full((heads_diff, 2, tok), -jnp.inf, jnp.float32),
        jnp.zeros((heads_diff, 2, tok), jnp.float32),
        jnp.zeros((heads_diff, 2, tok, VDIM), jnp.float32),
    )
    carry = start_state
    keys = lax.all_gather(k_diff, "sp", axis=0, tiled=True)
    values = lax.all_gather(v_diff, "sp", axis=0, tiled=True)
    rows = keys.shape[0]
    step = math.gcd(rows, 1024)
    key_blocks = keys.reshape(rows // step, step, heads_diff, 2, HEAD)
    value_blocks = values.reshape(rows // step, step, heads_diff, VDIM)

    def one(state, block):
        top, total, acc = state
        key_part, value_part = block
        scores = (
            jnp.einsum("qhmd,khmd->hmqk", q_four, key_part, preferred_element_type=jnp.float32)
            * scale
        )
        new_top = jnp.maximum(top, jnp.max(scores, axis=-1))
        expo = jnp.exp(scores - new_top[..., None])
        fade = jnp.exp(top - new_top)
        total = total * fade + jnp.sum(expo, axis=-1)
        acc = acc * fade[..., None] + jnp.einsum(
            "hmqk,khe->hmqe",
            expo.astype(jnp.bfloat16),
            value_part,
            preferred_element_type=jnp.float32,
        )
        return ((new_top, total, acc), None)

    carry, _ = lax.scan(one, carry, (key_blocks, value_blocks))
    _, total, acc = carry
    attention_maps = acc / total[..., None]
    difference_output = attention_maps[:, 0] - lam[:, None, None] * attention_maps[:, 1]
    differential_output = root_mean_square_rows(difference_output, output_norm_gain).astype(
        jnp.bfloat16
    )
    differential_output = jnp.transpose(differential_output, (1, 0, 2)).reshape(
        tok, heads_diff * VDIM
    )
    padded = padded_2(kv_win, (("sp", 0),), WINDOW)
    nblocks = tok // WINDOW
    blocks = padded.reshape(nblocks + 2, WINDOW, 2 * HEAD)
    band = jnp.concatenate([blocks[:-2], blocks[1:-1], blocks[2:]], axis=1)
    q_blocks = q_win.reshape(nblocks, WINDOW, heads_win, HEAD)
    scores = (
        jnp.einsum("nqhd,nkd->nhqk", q_blocks, band[..., :HEAD], preferred_element_type=jnp.float32)
        * scale
    )
    q_index = jnp.arange(WINDOW)
    k_index = jnp.arange(3 * WINDOW)
    relative = k_index[None, :] - WINDOW - q_index[:, None]
    first_key = lax.axis_index("sp") * tok - WINDOW
    key_pos = first_key + jnp.arange(nblocks)[:, None] * WINDOW + k_index[None, :]
    inside = (key_pos >= 0) & (key_pos < tok * lax.axis_size("sp"))
    valid = (jnp.abs(relative) <= WINDOW)[None] & inside[:, None, :]
    scores = jnp.where(valid[:, None], scores, -jnp.inf)
    sink_logit = sink[None, :, None, None]
    top_win = jnp.maximum(jnp.max(scores, axis=-1, keepdims=True), sink_logit)
    expo = jnp.exp(scores - top_win)
    weights = expo / (jnp.sum(expo, axis=-1, keepdims=True) + jnp.exp(sink_logit - top_win))
    y_win = jnp.einsum(
        "nhqk,nkd->nqhd",
        weights.astype(jnp.bfloat16),
        band[..., HEAD:],
        preferred_element_type=jnp.float32,
    ).astype(jnp.bfloat16)
    y_win = y_win.reshape(tok, heads_win * HEAD)
    summed = jnp.dot(differential_output, proj_diff, preferred_element_type=jnp.float32)
    return lax.psum_scatter(
        (summed + jnp.dot(y_win, proj_win, preferred_element_type=jnp.float32)).astype(
            jnp.bfloat16
        ),
        "tp",
        scatter_dimension=0,
        tiled=True,
    )


def row_of(i, s, x, nx, rows):
    slot = (i // nx) ^ s
    side = (i % nx) ^ x
    early = rows // WINDOW // nx - 1
    row = jnp.where(slot < early, side * early + slot, nx * early + side) * WINDOW
    return pl.multiple_of(row, WINDOW)


def attention_kernel(
    place, lam_a, lam_b, sink_a, sink_b, gain, q_ref, own_ref, oth_ref, *outs, nx, flip
):
    step = pl.program_id(0)
    s, x, c = place[0], place[1], place[2]
    rows = own_ref.shape[0]
    blocks = 2
    scale = HEAD**-0.5
    swapped = ((s // 2) ^ c) == 1
    lam = jnp.where(swapped, lam_b[s % 2], lam_a[s % 2])
    sinks = [
        jnp.where(swapped, sink_b[(s % 2) * 2 + h], sink_a[(s % 2) * 2 + h]) for h in range(2)
    ]
    nt = (((1,), (1,)), ((), ()))
    at = [((step * blocks + j) ^ s) * nx + (x ^ flip) for j in range(blocks)]
    places = [row_of(i, s, x, nx, rows) for i in at]

    def q_of(lanes):
        return jnp.concatenate([q_ref[pl.ds(r, WINDOW), lanes] for r in places], axis=0)

    maps = []
    for m in range(2):
        lanes = slice(m * HEAD, (m + 1) * HEAD)
        q = q_of(lanes)
        sa = lax.dot_general(q, own_ref[:, lanes], nt, preferred_element_type=F32)
        sb = lax.dot_general(q, oth_ref[:, lanes], nt, preferred_element_type=F32)
        top = jnp.maximum(
            jnp.max(sa, axis=-1, keepdims=True), jnp.max(sb, axis=-1, keepdims=True)
        )
        top = top * (scale * LOG2E)
        ea = jnp.exp2(sa * (scale * LOG2E) - top)
        eb = jnp.exp2(sb * (scale * LOG2E) - top)
        total = jnp.sum(ea, axis=-1, keepdims=True) + jnp.sum(eb, axis=-1, keepdims=True)
        acc = jnp.dot(ea.astype(BF), own_ref[:, 256:512], preferred_element_type=F32)
        acc = acc + jnp.dot(eb.astype(BF), oth_ref[:, 256:512], preferred_element_type=F32)
        maps.append(acc / total)
    d = maps[0] - lam * maps[1]
    y = d * lax.rsqrt(jnp.mean(d * d, axis=-1, keepdims=True) + EPS) * gain[...]
    y = y.astype(BF)
    last = rows // WINDOW - 1
    kw = slice(512, 512 + HEAD)
    vw = slice(512 + HEAD, 512 + 2 * HEAD)
    q_at = lax.broadcasted_iota(jnp.int32, (WINDOW, WINDOW), 0)
    k_at = lax.broadcasted_iota(jnp.int32, (WINDOW, WINDOW), 1)
    wins = []
    for i, r_own in zip(at, places):
        before = i - 1 + c
        after = i + c
        r_bef = row_of(jnp.maximum(before, 0), s, x, nx, rows)
        r_aft = row_of(jnp.minimum(after, last), s, x, nx, rows)
        k0 = oth_ref[pl.ds(r_bef, WINDOW), kw]
        k1 = own_ref[pl.ds(r_own, WINDOW), kw]
        k2 = oth_ref[pl.ds(r_aft, WINDOW), kw]
        v0 = oth_ref[pl.ds(r_bef, WINDOW), vw]
        v1 = own_ref[pl.ds(r_own, WINDOW), vw]
        v2 = oth_ref[pl.ds(r_aft, WINDOW), vw]
        ok0 = (k_at >= q_at) & (before >= 0)
        ok2 = (k_at <= q_at) & (after <= last)
        for h in range(2):
            q = q_ref[pl.ds(r_own, WINDOW), 256 + h * HEAD : 256 + (h + 1) * HEAD]
            z0 = lax.dot_general(q, k0, nt, preferred_element_type=F32) * scale
            z1 = lax.dot_general(q, k1, nt, preferred_element_type=F32) * scale
            z2 = lax.dot_general(q, k2, nt, preferred_element_type=F32) * scale
            z0 = jnp.where(ok0, z0, -jnp.inf)
            z2 = jnp.where(ok2, z2, -jnp.inf)
            top = jnp.max(jnp.maximum(jnp.maximum(z0, z1), z2), axis=-1, keepdims=True)
            top = jnp.maximum(top, sinks[h])
            e0, e1, e2 = jnp.exp(z0 - top), jnp.exp(z1 - top), jnp.exp(z2 - top)
            total = jnp.sum(e0 + e1 + e2, axis=-1, keepdims=True) + jnp.exp(sinks[h] - top)
            w = 1.0 / total
            acc = jnp.dot((e0 * w).astype(BF), v0, preferred_element_type=F32)
            acc = acc + jnp.dot((e1 * w).astype(BF), v1, preferred_element_type=F32)
            acc = acc + jnp.dot((e2 * w).astype(BF), v2, preferred_element_type=F32)
            wins.append(acc.astype(BF))
    for t in range(len(outs) // blocks):

        @pl.when(step == t)
        def _(t=t):
            for j in range(blocks):
                out = outs[t * blocks + j]
                out[:, 0:VDIM] = y[j * WINDOW : (j + 1) * WINDOW]
                out[:, VDIM : VDIM + HEAD] = wins[2 * j]
                out[:, VDIM + HEAD : VDIM + 2 * HEAD] = wins[2 * j + 1]


def attention(place, scalars, gain, q, own, oth, sp, nx, flip):
    rows = own.shape[0]
    smem = pl.BlockSpec(memory_space=pltpu.SMEM)
    whole = pl.BlockSpec(own.shape, lambda i: (0, 0))
    block = pl.BlockSpec((WINDOW, 2 * VDIM), lambda i: (0, 0))

    def kernel(*refs):
        attention_kernel(*refs, nx=nx, flip=flip)

    return pl.pallas_call(
        kernel,
        grid=(sp // 2,),
        in_specs=[smem] * 5
        + [pl.BlockSpec((1, VDIM), lambda i: (0, 0)), pl.BlockSpec(q.shape, lambda i: (0, 0))]
        + [whole, whole],
        out_specs=[block] * sp,
        out_shape=[jax.ShapeDtypeStruct((WINDOW, 2 * VDIM), BF)] * sp,
        compiler_params=pltpu.CompilerParams(dimension_semantics=("arbitrary",)),
        cost_estimate=pl.CostEstimate(
            flops=4 * sp * WINDOW * rows * 2 * 384,
            bytes_accessed=4 * 2**20,
            transcendentals=0,
        ),
        name="attend",
    )(place, *scalars, gain, q, own, oth)


def assemble(scratch, row, pieces, g, c):
    size = pieces[0].shape[0]
    parts = []
    for p in pieces:
        for lo in range(0, p.shape[0], size):
            parts.append(p[lo : lo + size, :])
    if len(parts) == 1:
        scratch[row : row + size, :] = parts[0]
        return
    for j, part in enumerate(parts):
        quarter = (g ^ (j & 1)) * 2 + (c ^ (j >> 1))
        scratch[pl.ds(pl.multiple_of(row + quarter * size, size), size), :] = part


ROWS = 256


def project_early(place, acts, own, pieces, split):
    rows = acts.shape[0]
    wide, cols = own.shape

    def kernel(place_ref, a0, a1, own_ref, *refs):
        (*ws, left, right, scratch) = refs

        @pl.when(pl.program_id(0) == 0)
        def _():
            assemble(scratch, 0, ws, place_ref[3], place_ref[2])

        total = jnp.dot(a0[...], own_ref[...], preferred_element_type=F32)
        total = total + jnp.dot(a1[...], scratch[...], preferred_element_type=F32)
        left[...] = total[:, :split]
        right[...] = total[:, split:]

    def chunk_of(k):
        return pl.BlockSpec((ROWS, wide), lambda m, at: (m, at[0] ^ k))

    whole = [pl.BlockSpec(p.shape, lambda m, at: (0, 0)) for p in (own, *pieces)]
    widths = (split, cols - split)
    return pl.pallas_call(
        kernel,
        grid_spec=pltpu.PrefetchScalarGridSpec(
            num_scalar_prefetch=1,
            grid=(rows // ROWS,),
            in_specs=[chunk_of(0), chunk_of(1), *whole],
            out_specs=[pl.BlockSpec((ROWS, w), lambda m, at: (m, 0)) for w in widths],
            scratch_shapes=[pltpu.VMEM((wide, cols), BF)],
        ),
        out_shape=[jax.ShapeDtypeStruct((rows, w), F32) for w in widths],
        compiler_params=pltpu.CompilerParams(dimension_semantics=("arbitrary",)),
        cost_estimate=pl.CostEstimate(
            flops=4 * rows * wide * cols, bytes_accessed=rows * cols * 8, transcendentals=0
        ),
        name="project",
    )(place, acts, acts, own, *pieces)


def project_rest(place, early, late, acc, chunks, begin, cols):
    wide = sum(p.shape[0] for p in chunks[0][0])
    steps = early.shape[0] // ROWS
    order = sorted(chunks)
    counts = [len(chunks[k][0]) for k in order]

    def kernel(place_ref, acc_ref, e2, e3, *refs):
        acts = refs[: len(order)]
        refs = refs[len(order) :]
        out, scratch = refs[-2], refs[-1]
        m = pl.program_id(0)

        @pl.when(m == 0)
        def _():
            at = 0
            for j, n in enumerate(counts):
                assemble(scratch, j * wide, refs[at : at + n], place_ref[3], place_ref[2])
                at += n

        def part(a, j):
            return jnp.dot(
                a[...], scratch[j * wide : (j + 1) * wide], preferred_element_type=F32
            )

        @pl.when(m < steps)
        def _():
            out[...] = (acc_ref[...] + part(e2, 2) + part(e3, 3)).astype(BF)

        @pl.when(m == steps)
        def _():
            total = part(acts[0], 0)
            for j in range(1, len(order)):
                total = total + part(acts[j], j)
            out[...] = total.astype(BF)

    def early_of(k):
        return pl.BlockSpec(
            (ROWS, wide), lambda m, at: (jnp.minimum(m, steps - 1), at[0] ^ k)
        )

    in_specs = [pl.BlockSpec((ROWS, cols), lambda m, at: (jnp.minimum(m, steps - 1), 0))]
    in_specs += [early_of(2), early_of(3)]
    in_specs += [pl.BlockSpec((ROWS, wide), lambda m, at, k=k: (0, at[0] ^ k)) for k in order]
    operands = [acc, early, early] + [late] * len(order)
    for k in order:
        pieces, start = chunks[k]
        for p in pieces:
            in_specs.append(
                pl.BlockSpec(
                    (pl.Element(p.shape[0]), pl.Element(cols)),
                    lambda m, at, lo=begin - start: (0, lo),
                )
                if p.shape[1] != cols
                else pl.BlockSpec(p.shape, lambda m, at: (0, 0))
            )
            operands.append(p)
    return pl.pallas_call(
        kernel,
        grid_spec=pltpu.PrefetchScalarGridSpec(
            num_scalar_prefetch=1,
            grid=(steps + 1,),
            in_specs=in_specs,
            out_specs=pl.BlockSpec((ROWS, cols), lambda m, at: (m, 0)),
            scratch_shapes=[pltpu.VMEM((len(order) * wide, cols), BF)],
        ),
        out_shape=jax.ShapeDtypeStruct((early.shape[0] + late.shape[0], cols), BF),
        compiler_params=pltpu.CompilerParams(dimension_semantics=("arbitrary",)),
        cost_estimate=pl.CostEstimate(
            flops=2 * (2 * early.shape[0] + 4 * late.shape[0]) * wide * cols,
            bytes_accessed=16 * 2**20,
            transcendentals=0,
        ),
        name="project",
    )(place, *operands)


def output_projection(place, heads, weights, first, count, kind):
    sp = len(heads)
    tile = OUT_TILE

    def kernel(place_ref, *refs):
        ys, ws, (out, ordered) = refs[:sp], refs[sp : sp + 4], refs[sp + 4 :]
        s, c = place_ref[0], place_ref[2]
        n = pl.program_id(0)

        @pl.when(n == 0)
        def _():
            for k, y in enumerate(ys):
                ordered[(s ^ k) ^ (2 * c)] = y[...]

        total = None
        for j, w in enumerate(ws):
            lanes = slice((j % 2) * VDIM, (j % 2 + 1) * VDIM)
            for local in range(2):
                part = jnp.dot(
                    ordered[(j // 2) * 2 + local, :, lanes],
                    w[local * VDIM : (local + 1) * VDIM],
                    preferred_element_type=F32,
                )
                total = part if total is None else total + part
        out[...] = total.astype(out.dtype)

    whole = pl.BlockSpec((WINDOW, 2 * VDIM), lambda n: (0, 0))
    in_specs = [pl.BlockSpec(memory_space=pltpu.SMEM)] + [whole] * sp
    in_specs += [pl.BlockSpec((2 * VDIM, tile), lambda n: (0, n + first))] * 4
    operands = [place, *heads, *weights]
    return pl.pallas_call(
        kernel,
        grid=(count,),
        in_specs=in_specs,
        out_specs=pl.BlockSpec((WINDOW, tile), lambda n: (0, n)),
        out_shape=jax.ShapeDtypeStruct((WINDOW, count * tile), kind),
        scratch_shapes=[pltpu.VMEM((sp, WINDOW, 2 * VDIM), BF)],
        compiler_params=pltpu.CompilerParams(dimension_semantics=("arbitrary",)),
        cost_estimate=pl.CostEstimate(
            flops=2 * WINDOW * 2048 * count * tile,
            bytes_accessed=2048 * count * tile * 2,
            transcendentals=0,
        ),
        name="output",
    )(*operands)


def chip_body(
    tokens,
    norm_gain,
    query_diff,
    key_diff,
    value_diff,
    lam,
    output_norm_gain,
    query_win,
    keyval_win,
    sink,
    proj_diff,
    proj_win,
):
    ng, sp, tp = (lax.axis_size(a) for a in AXES)
    nx = tp // 2
    g, s, t = (lax.axis_index(a) for a in AXES)
    x, c = t // 2, t % 2

    def send(value, target, only=None):
        pairs = []
        for i in range(ng * sp * tp):
            at = (i // (sp * tp), i // tp % sp, i % tp // 2, i % 2)
            if only is None or only(*at):
                a, b, d, e = target(*at)
                pairs.append((i, ((a * sp + b) * nx + d) * 2 + e))
        return lax.ppermute(value, AXES, pairs)

    def over_core(v):
        return send(v, lambda a, b, d, e: (a, b, d, e ^ 1))

    def over_x(v):
        return send(v, lambda a, b, d, e: (a, b, d ^ 1, e))

    def over_y(v):
        return send(v, lambda a, b, d, e: (a ^ 1, b, d, e))

    def over_z(v, k):
        return send(v, lambda a, b, d, e: (a, b ^ k, d, e))

    def mids(v, k):
        return send(v, lambda a, b, d, e: (a, b ^ k, d, e), lambda a, b, d, e: b in (1, 2))

    mid = (s == 1) | (s == 2)
    normed = root_mean_square_rows(tokens.astype(F32), norm_gain).astype(BF)
    one = over_z(normed, 1)
    near = mids(normed, 3)
    tx0 = over_x(normed)
    far = mids(near, 1)
    cross = mids(one, 3)
    tx1 = over_x(one)
    last = mids(cross, 1)
    slot2 = jnp.where(mid, cross, far)
    tx2 = over_x(slot2)
    slot3 = jnp.where(mid, near, last)
    tx3 = over_x(slot3)
    early = jnp.concatenate([normed, one, slot2, tx0, tx1, tx2], axis=0)
    late = jnp.concatenate([slot3, tx3], axis=0)

    rows_w = query_diff.shape[0]
    quarter = rows_w // 4

    def pack(lo, size, head):
        parts = []
        for w in (key_diff, value_diff, query_diff, query_win):
            parts.append(lax.dynamic_slice(w, (lo, head * VDIM), (size, VDIM)))
        return jnp.concatenate(parts, axis=1)

    def kv_pack(lo, size, h):
        kv = lax.dynamic_slice(keyval_win, (nx * x + h // 2, lo, 0), (1, size, 2 * HEAD))
        return kv[0]

    def with_kv(four, kv):
        return jnp.concatenate([four[:, : 2 * VDIM], kv, four[:, 2 * VDIM :]], axis=1)

    mine_lo = (g * 2 + c) * quarter
    give_lo = (g * 2 + 1 - c) * quarter
    give = jnp.stack([pack(give_lo, quarter, 0), pack(give_lo, quarter, 1)])
    keep = jnp.stack([pack(mine_lo, quarter, 0), pack(mine_lo, quarter, 1)])
    both = jnp.concatenate([keep, over_core(give)], axis=0)
    local = pack(0, rows_w, s % 2)
    moved = send(local, lambda a, b, d, e: (a, b, d, e ^ 1), lambda a, b, d, e: e == b // 2)
    own = with_kv(jnp.where(c == s // 2, local, moved), kv_pack(0, rows_w, s))

    place = jnp.stack([s, x, c, g]).astype(jnp.int32)

    def package(k):
        h = s ^ k
        pick = lax.dynamic_index_in_dim(both, ((h // 2) ^ c) * 2 + h % 2, 0, keepdims=False)
        return pick, kv_pack(mine_lo, quarter, h)

    def chunk(part, k):
        got = over_z(part, k)
        got_y = over_y(got)
        return [got, got_y, over_core(jnp.concatenate([got, got_y], axis=0))]

    w1 = chunk(with_kv(*package(1)), 1)
    w3 = chunk(with_kv(*package(3)), 3)
    four, kv = package(2)
    w2a = chunk(jnp.concatenate([four[:, : 2 * VDIM], kv], axis=1), 2)
    w2b = chunk(four[:, 2 * VDIM :], 2)
    split = 3 * VDIM
    acc_kv, acc_q = project_early(place, early, own, w1, split)
    every = {0: ([own], 0), 1: (w1, 0), 3: (w3, 0)}
    kv_own = project_rest(place, early, late, acc_kv, every | {2: (w2a, 0)}, 0, split)
    kv_oth = over_core(kv_own)
    queries = project_rest(
        place, early, late, acc_q, every | {2: (w2b, split)}, split, own.shape[1] - split
    )

    scalars = (lam, over_core(lam), sink, over_core(sink))
    gain = output_norm_gain.reshape(1, VDIM)
    weights = [proj_diff, proj_win, over_core(proj_diff), over_core(proj_win)]

    def spread(ys):
        return [ys[0]] + [over_z(ys[k], k) for k in range(1, sp)]

    def attend(flip):
        return attention(place, scalars, gain, queries, kv_own, kv_oth, sp, nx, flip)

    far_heads = spread(attend(1))
    y_near = attend(0)
    near_heads = spread(y_near)
    received = []
    tiles = proj_diff.shape[1] // OUT_TILE
    for begin, end in ((0, 1), (1, tiles)):
        part = output_projection(place, far_heads, weights, begin, end - begin, BF)
        received.append(over_x(part))
    kept = output_projection(place, near_heads, weights, 0, tiles, F32)
    return (kept + jnp.concatenate(received, axis=1).astype(F32)).astype(BF)


def solution(mesh):
    placed = (
        P(("grp", "sp", "tp"), None),
        P(),
        P("sp", "tp"),
        P("sp", "tp"),
        P("sp", "tp"),
        P("tp"),
        P(),
        P("sp", "tp"),
        P(None, "sp", None),
        P("tp"),
        P("tp", None),
        P("tp", None),
    )
    sizes = dict(mesh.shape)

    def body(*args):
        tokens, lam, sink = args[0], args[5], args[9]
        fits = (
            sizes["grp"] == 2
            and sizes["sp"] == 4
            and sizes["tp"] == 4
            and tokens.shape[0] == WINDOW
            and lam.shape[0] == 2
            and sink.shape[0] == 4
        )
        return (chip_body if fits else general_body)(*args)

    return jax.shard_map(
        body, mesh=mesh, in_specs=placed, out_specs=P(("grp", "sp", "tp"), None), check_vma=False
    )
```

```python
import math

import jax
import jax.numpy as jnp
from jax import lax
from jax.experimental import pallas as pl
from jax.experimental.pallas import tpu as pltpu
from jax.sharding import PartitionSpec as P


HEAD = 128
WIN_HEADS = 16
KV_HEADS = 4
WINDOW = 128
VDIM = 256
EPS = 1e-06
LOG2E = math.log2(math.e)
AXES = ("grp", "sp", "tp")

OUT_TILE = 1024
BF = jnp.bfloat16
F32 = jnp.float32


def padded_2(x, sides, width):
    for axis, dim in sides:
        devices, length = (lax.axis_size(axis), x.shape[dim])
        up = [(i, (i + 1) % devices) for i in range(devices - 1)]
        down = [(j, i) for i, j in up]
        last = lax.slice_in_dim(x, length - width, length, axis=dim)
        first = lax.slice_in_dim(x, 0, width, axis=dim)
        before = lax.ppermute(last, axis, up)
        after = lax.ppermute(first, axis, down)
        x = jnp.concatenate([before, x, after], axis=dim)
    return x


def root_mean_square_rows(values, gain):
    return values * lax.rsqrt(jnp.mean(values * values, axis=-1, keepdims=True) + EPS) * gain


def general_body(
    tokens,
    norm_gain,
    query_diff,
    key_diff,
    value_diff,
    lam,
    output_norm_gain,
    query_win,
    keyval_win,
    sink,
    proj_diff,
    proj_win,
):
    normed = root_mean_square_rows(tokens.astype(jnp.float32), norm_gain).astype(jnp.bfloat16)
    heads_diff = lam.shape[0]
    heads_win = sink.shape[0]
    group = WIN_HEADS // KV_HEADS
    kv_index = lax.axis_index("tp") * heads_win // group
    kv_local = lax.dynamic_index_in_dim(keyval_win, kv_index, 0, keepdims=False)
    pieces = [query_diff, key_diff, value_diff, query_win, kv_local]
    stacked = jnp.concatenate(pieces, axis=1)
    whole = lax.all_gather(stacked, "sp", axis=0, tiled=True)
    projected = jnp.dot(
        lax.all_gather(normed, "tp", axis=0, tiled=True), whole, preferred_element_type=jnp.float32
    )
    projected = projected.astype(jnp.bfloat16)
    output_list = []
    offset = 0
    for piece in pieces:
        output_list.append(projected[:, offset : offset + piece.shape[1]])
        offset = offset + piece.shape[1]
    q_diff, k_diff, v_diff, q_win, kv_win = output_list
    tok = projected.shape[0]
    scale = HEAD ** (-0.5)
    q_four = q_diff.reshape(tok, heads_diff, 2, HEAD)
    start_state = (
        jnp.full((heads_diff, 2, tok), -jnp.inf, jnp.float32),
        jnp.zeros((heads_diff, 2, tok), jnp.float32),
        jnp.zeros((heads_diff, 2, tok, VDIM), jnp.float32),
    )
    carry = start_state
    keys = lax.all_gather(k_diff, "sp", axis=0, tiled=True)
    values = lax.all_gather(v_diff, "sp", axis=0, tiled=True)
    rows = keys.shape[0]
    step = math.gcd(rows, 1024)
    key_blocks = keys.reshape(rows // step, step, heads_diff, 2, HEAD)
    value_blocks = values.reshape(rows // step, step, heads_diff, VDIM)

    def one(state, block):
        top, total, acc = state
        key_part, value_part = block
        scores = (
            jnp.einsum("qhmd,khmd->hmqk", q_four, key_part, preferred_element_type=jnp.float32)
            * scale
        )
        new_top = jnp.maximum(top, jnp.max(scores, axis=-1))
        expo = jnp.exp(scores - new_top[..., None])
        fade = jnp.exp(top - new_top)
        total = total * fade + jnp.sum(expo, axis=-1)
        acc = acc * fade[..., None] + jnp.einsum(
            "hmqk,khe->hmqe",
            expo.astype(jnp.bfloat16),
            value_part,
            preferred_element_type=jnp.float32,
        )
        return ((new_top, total, acc), None)

    carry, _ = lax.scan(one, carry, (key_blocks, value_blocks))
    _, total, acc = carry
    attention_maps = acc / total[..., None]
    difference_output = attention_maps[:, 0] - lam[:, None, None] * attention_maps[:, 1]
    differential_output = root_mean_square_rows(difference_output, output_norm_gain).astype(
        jnp.bfloat16
    )
    differential_output = jnp.transpose(differential_output, (1, 0, 2)).reshape(
        tok, heads_diff * VDIM
    )
    padded = padded_2(kv_win, (("sp", 0),), WINDOW)
    nblocks = tok // WINDOW
    blocks = padded.reshape(nblocks + 2, WINDOW, 2 * HEAD)
    band = jnp.concatenate([blocks[:-2], blocks[1:-1], blocks[2:]], axis=1)
    q_blocks = q_win.reshape(nblocks, WINDOW, heads_win, HEAD)
    scores = (
        jnp.einsum("nqhd,nkd->nhqk", q_blocks, band[..., :HEAD], preferred_element_type=jnp.float32)
        * scale
    )
    q_index = jnp.arange(WINDOW)
    k_index = jnp.arange(3 * WINDOW)
    relative = k_index[None, :] - WINDOW - q_index[:, None]
    first_key = lax.axis_index("sp") * tok - WINDOW
    key_pos = first_key + jnp.arange(nblocks)[:, None] * WINDOW + k_index[None, :]
    inside = (key_pos >= 0) & (key_pos < tok * lax.axis_size("sp"))
    valid = (jnp.abs(relative) <= WINDOW)[None] & inside[:, None, :]
    scores = jnp.where(valid[:, None], scores, -jnp.inf)
    sink_logit = sink[None, :, None, None]
    top_win = jnp.maximum(jnp.max(scores, axis=-1, keepdims=True), sink_logit)
    expo = jnp.exp(scores - top_win)
    weights = expo / (jnp.sum(expo, axis=-1, keepdims=True) + jnp.exp(sink_logit - top_win))
    y_win = jnp.einsum(
        "nhqk,nkd->nqhd",
        weights.astype(jnp.bfloat16),
        band[..., HEAD:],
        preferred_element_type=jnp.float32,
    ).astype(jnp.bfloat16)
    y_win = y_win.reshape(tok, heads_win * HEAD)
    summed = jnp.dot(differential_output, proj_diff, preferred_element_type=jnp.float32)
    return lax.psum_scatter(
        (summed + jnp.dot(y_win, proj_win, preferred_element_type=jnp.float32)).astype(
            jnp.bfloat16
        ),
        "tp",
        scatter_dimension=0,
        tiled=True,
    )


def row_of(i, s, x, nx, rows):
    slot = (i // nx) ^ s
    side = (i % nx) ^ x
    early = rows // WINDOW // nx - 1
    row = jnp.where(slot < early, side * early + slot, nx * early + side) * WINDOW
    return pl.multiple_of(row, WINDOW)


def attention_kernel(
    place, lam_a, lam_b, sink_a, sink_b, gain, q_ref, own_ref, oth_ref, *outs, nx, flip
):
    step = pl.program_id(0)
    s, x, c = place[0], place[1], place[2]
    rows = own_ref.shape[0]
    blocks = 2
    scale = HEAD**-0.5
    swapped = ((s // 2) ^ c) == 1
    lam = jnp.where(swapped, lam_b[s % 2], lam_a[s % 2])
    sinks = [
        jnp.where(swapped, sink_b[(s % 2) * 2 + h], sink_a[(s % 2) * 2 + h]) for h in range(2)
    ]
    nt = (((1,), (1,)), ((), ()))
    at = [((step * blocks + j) ^ s) * nx + (x ^ flip) for j in range(blocks)]
    places = [row_of(i, s, x, nx, rows) for i in at]

    def q_of(lanes):
        return jnp.concatenate([q_ref[pl.ds(r, WINDOW), lanes] for r in places], axis=0)

    maps = []
    for m in range(2):
        lanes = slice(m * HEAD, (m + 1) * HEAD)
        q = q_of(lanes)
        sa = lax.dot_general(q, own_ref[:, lanes], nt, preferred_element_type=F32)
        sb = lax.dot_general(q, oth_ref[:, lanes], nt, preferred_element_type=F32)
        top = jnp.maximum(
            jnp.max(sa, axis=-1, keepdims=True), jnp.max(sb, axis=-1, keepdims=True)
        )
        top = top * (scale * LOG2E)
        ea = jnp.exp2(sa * (scale * LOG2E) - top)
        eb = jnp.exp2(sb * (scale * LOG2E) - top)
        total = jnp.sum(ea, axis=-1, keepdims=True) + jnp.sum(eb, axis=-1, keepdims=True)
        acc = jnp.dot(ea.astype(BF), own_ref[:, 256:512], preferred_element_type=F32)
        acc = acc + jnp.dot(eb.astype(BF), oth_ref[:, 256:512], preferred_element_type=F32)
        maps.append(acc / total)
    d = maps[0] - lam * maps[1]
    y = d * lax.rsqrt(jnp.mean(d * d, axis=-1, keepdims=True) + EPS) * gain[...]
    y = y.astype(BF)
    last = rows // WINDOW - 1
    kw = slice(512, 512 + HEAD)
    vw = slice(512 + HEAD, 512 + 2 * HEAD)
    q_at = lax.broadcasted_iota(jnp.int32, (WINDOW, WINDOW), 0)
    k_at = lax.broadcasted_iota(jnp.int32, (WINDOW, WINDOW), 1)
    wins = []
    for i, r_own in zip(at, places):
        before = i - 1 + c
        after = i + c
        r_bef = row_of(jnp.maximum(before, 0), s, x, nx, rows)
        r_aft = row_of(jnp.minimum(after, last), s, x, nx, rows)
        k0 = oth_ref[pl.ds(r_bef, WINDOW), kw]
        k1 = own_ref[pl.ds(r_own, WINDOW), kw]
        k2 = oth_ref[pl.ds(r_aft, WINDOW), kw]
        v0 = oth_ref[pl.ds(r_bef, WINDOW), vw]
        v1 = own_ref[pl.ds(r_own, WINDOW), vw]
        v2 = oth_ref[pl.ds(r_aft, WINDOW), vw]
        ok0 = (k_at >= q_at) & (before >= 0)
        ok2 = (k_at <= q_at) & (after <= last)
        for h in range(2):
            q = q_ref[pl.ds(r_own, WINDOW), 256 + h * HEAD : 256 + (h + 1) * HEAD]
            z0 = lax.dot_general(q, k0, nt, preferred_element_type=F32) * scale
            z1 = lax.dot_general(q, k1, nt, preferred_element_type=F32) * scale
            z2 = lax.dot_general(q, k2, nt, preferred_element_type=F32) * scale
            z0 = jnp.where(ok0, z0, -jnp.inf)
            z2 = jnp.where(ok2, z2, -jnp.inf)
            top = jnp.max(jnp.maximum(jnp.maximum(z0, z1), z2), axis=-1, keepdims=True)
            top = jnp.maximum(top, sinks[h])
            e0, e1, e2 = jnp.exp(z0 - top), jnp.exp(z1 - top), jnp.exp(z2 - top)
            total = jnp.sum(e0 + e1 + e2, axis=-1, keepdims=True) + jnp.exp(sinks[h] - top)
            w = 1.0 / total
            acc = jnp.dot((e0 * w).astype(BF), v0, preferred_element_type=F32)
            acc = acc + jnp.dot((e1 * w).astype(BF), v1, preferred_element_type=F32)
            acc = acc + jnp.dot((e2 * w).astype(BF), v2, preferred_element_type=F32)
            wins.append(acc.astype(BF))
    for t in range(len(outs) // blocks):

        @pl.when(step == t)
        def _(t=t):
            for j in range(blocks):
                out = outs[t * blocks + j]
                out[:, 0:VDIM] = y[j * WINDOW : (j + 1) * WINDOW]
                out[:, VDIM : VDIM + HEAD] = wins[2 * j]
                out[:, VDIM + HEAD : VDIM + 2 * HEAD] = wins[2 * j + 1]


def attention(place, scalars, gain, q, own, oth, sp, nx, flip):
    rows = own.shape[0]
    smem = pl.BlockSpec(memory_space=pltpu.SMEM)
    whole = pl.BlockSpec(own.shape, lambda i: (0, 0))
    block = pl.BlockSpec((WINDOW, 2 * VDIM), lambda i: (0, 0))

    def kernel(*refs):
        attention_kernel(*refs, nx=nx, flip=flip)

    return pl.pallas_call(
        kernel,
        grid=(sp // 2,),
        in_specs=[smem] * 5
        + [pl.BlockSpec((1, VDIM), lambda i: (0, 0)), pl.BlockSpec(q.shape, lambda i: (0, 0))]
        + [whole, whole],
        out_specs=[block] * sp,
        out_shape=[jax.ShapeDtypeStruct((WINDOW, 2 * VDIM), BF)] * sp,
        compiler_params=pltpu.CompilerParams(
            dimension_semantics=("arbitrary",), vmem_limit_bytes=20 * 2**20
        ),
        cost_estimate=pl.CostEstimate(
            flops=4 * sp * WINDOW * rows * 2 * 384,
            bytes_accessed=4 * 2**20,
            transcendentals=0,
        ),
        name="attend",
    )(place, *scalars, gain, q, own, oth)


def assemble(scratch, row, pieces, g, c):
    size = pieces[0].shape[0]
    parts = []
    for p in pieces:
        for lo in range(0, p.shape[0], size):
            parts.append(p[lo : lo + size, :])
    if len(parts) == 1:
        scratch[row : row + size, :] = parts[0]
        return
    for j, part in enumerate(parts):
        quarter = (g ^ (j & 1)) * 2 + (c ^ (j >> 1))
        scratch[pl.ds(pl.multiple_of(row + quarter * size, size), size), :] = part


ROWS = 256


def project_early(place, acts, own, pieces, split):
    rows = acts.shape[0]
    wide, cols = own.shape

    def kernel(place_ref, a0, a1, own_ref, *refs):
        (*ws, left, right, scratch) = refs

        @pl.when(pl.program_id(0) == 0)
        def _():
            assemble(scratch, 0, ws, place_ref[3], place_ref[2])

        total = jnp.dot(a0[...], own_ref[...], preferred_element_type=F32)
        total = total + jnp.dot(a1[...], scratch[...], preferred_element_type=F32)
        left[...] = total[:, :split]
        right[...] = total[:, split:]

    def chunk_of(k):
        return pl.BlockSpec((ROWS, wide), lambda m, at: (m, at[0] ^ k))

    whole = [pl.BlockSpec(p.shape, lambda m, at: (0, 0)) for p in (own, *pieces)]
    widths = (split, cols - split)
    return pl.pallas_call(
        kernel,
        grid_spec=pltpu.PrefetchScalarGridSpec(
            num_scalar_prefetch=1,
            grid=(rows // ROWS,),
            in_specs=[chunk_of(0), chunk_of(1), *whole],
            out_specs=[pl.BlockSpec((ROWS, w), lambda m, at: (m, 0)) for w in widths],
            scratch_shapes=[pltpu.VMEM((wide, cols), BF)],
        ),
        out_shape=[jax.ShapeDtypeStruct((rows, w), F32) for w in widths],
        compiler_params=pltpu.CompilerParams(
            dimension_semantics=("arbitrary",), vmem_limit_bytes=26 * 2**20
        ),
        cost_estimate=pl.CostEstimate(
            flops=4 * rows * wide * cols, bytes_accessed=rows * cols * 8, transcendentals=0
        ),
        name="project",
    )(place, acts, acts, own, *pieces)


def project_rest(place, early, late, acc, chunks, begin, cols):
    wide = sum(p.shape[0] for p in chunks[0][0])
    steps = early.shape[0] // ROWS
    order = sorted(chunks)
    counts = [len(chunks[k][0]) for k in order]

    def kernel(place_ref, acc_ref, e2, e3, *refs):
        acts = refs[: len(order)]
        refs = refs[len(order) :]
        out, scratch = refs[-2], refs[-1]
        m = pl.program_id(0)

        @pl.when(m == 0)
        def _():
            at = 0
            for j, n in enumerate(counts):
                assemble(scratch, j * wide, refs[at : at + n], place_ref[3], place_ref[2])
                at += n

        def part(a, j):
            return jnp.dot(
                a[...], scratch[j * wide : (j + 1) * wide], preferred_element_type=F32
            )

        @pl.when(m < steps)
        def _():
            out[...] = (acc_ref[...] + part(e2, 2) + part(e3, 3)).astype(BF)

        @pl.when(m == steps)
        def _():
            total = part(acts[0], 0)
            for j in range(1, len(order)):
                total = total + part(acts[j], j)
            out[...] = total.astype(BF)

    def early_of(k):
        return pl.BlockSpec(
            (ROWS, wide), lambda m, at: (jnp.minimum(m, steps - 1), at[0] ^ k)
        )

    in_specs = [pl.BlockSpec((ROWS, cols), lambda m, at: (jnp.minimum(m, steps - 1), 0))]
    in_specs += [early_of(2), early_of(3)]
    in_specs += [pl.BlockSpec((ROWS, wide), lambda m, at, k=k: (0, at[0] ^ k)) for k in order]
    operands = [acc, early, early] + [late] * len(order)
    for k in order:
        pieces, start = chunks[k]
        for p in pieces:
            in_specs.append(
                pl.BlockSpec(
                    (pl.Element(p.shape[0]), pl.Element(cols)),
                    lambda m, at, lo=begin - start: (0, lo),
                )
                if p.shape[1] != cols
                else pl.BlockSpec(p.shape, lambda m, at: (0, 0))
            )
            operands.append(p)
    return pl.pallas_call(
        kernel,
        grid_spec=pltpu.PrefetchScalarGridSpec(
            num_scalar_prefetch=1,
            grid=(steps + 1,),
            in_specs=in_specs,
            out_specs=pl.BlockSpec((ROWS, cols), lambda m, at: (m, 0)),
            scratch_shapes=[pltpu.VMEM((len(order) * wide, cols), BF)],
        ),
        out_shape=jax.ShapeDtypeStruct((early.shape[0] + late.shape[0], cols), BF),
        compiler_params=pltpu.CompilerParams(
            dimension_semantics=("arbitrary",), vmem_limit_bytes=36 * 2**20
        ),
        cost_estimate=pl.CostEstimate(
            flops=2 * (2 * early.shape[0] + 4 * late.shape[0]) * wide * cols,
            bytes_accessed=16 * 2**20,
            transcendentals=0,
        ),
        name="project",
    )(place, *operands)


def output_projection(place, heads, weights, first, count, kind):
    sp = len(heads)
    tile = OUT_TILE

    def kernel(place_ref, *refs):
        ys, ws, (out, ordered) = refs[:sp], refs[sp : sp + 4], refs[sp + 4 :]
        s, c = place_ref[0], place_ref[2]
        n = pl.program_id(0)

        @pl.when(n == 0)
        def _():
            for k, y in enumerate(ys):
                ordered[(s ^ k) ^ (2 * c)] = y[...]

        total = None
        for j, w in enumerate(ws):
            lanes = slice((j % 2) * VDIM, (j % 2 + 1) * VDIM)
            for local in range(2):
                part = jnp.dot(
                    ordered[(j // 2) * 2 + local, :, lanes],
                    w[local * VDIM : (local + 1) * VDIM],
                    preferred_element_type=F32,
                )
                total = part if total is None else total + part
        out[...] = total.astype(out.dtype)

    whole = pl.BlockSpec((WINDOW, 2 * VDIM), lambda n: (0, 0))
    in_specs = [pl.BlockSpec(memory_space=pltpu.SMEM)] + [whole] * sp
    in_specs += [pl.BlockSpec((2 * VDIM, tile), lambda n: (0, n + first))] * 4
    operands = [place, *heads, *weights]
    return pl.pallas_call(
        kernel,
        grid=(count,),
        in_specs=in_specs,
        out_specs=pl.BlockSpec((WINDOW, tile), lambda n: (0, n)),
        out_shape=jax.ShapeDtypeStruct((WINDOW, count * tile), kind),
        scratch_shapes=[pltpu.VMEM((sp, WINDOW, 2 * VDIM), BF)],
        compiler_params=pltpu.CompilerParams(
            dimension_semantics=("arbitrary",), vmem_limit_bytes=16 * 2**20
        ),
        cost_estimate=pl.CostEstimate(
            flops=2 * WINDOW * 2048 * count * tile,
            bytes_accessed=2048 * count * tile * 2,
            transcendentals=0,
        ),
        name="output",
    )(*operands)


def chip_body(
    tokens,
    norm_gain,
    query_diff,
    key_diff,
    value_diff,
    lam,
    output_norm_gain,
    query_win,
    keyval_win,
    sink,
    proj_diff,
    proj_win,
):
    ng, sp, tp = (lax.axis_size(a) for a in AXES)
    nx = tp // 2
    g, s, t = (lax.axis_index(a) for a in AXES)
    x, c = t // 2, t % 2

    def send(value, target, only=None):
        pairs = []
        for i in range(ng * sp * tp):
            at = (i // (sp * tp), i // tp % sp, i % tp // 2, i % 2)
            if only is None or only(*at):
                a, b, d, e = target(*at)
                pairs.append((i, ((a * sp + b) * nx + d) * 2 + e))
        return lax.ppermute(value, AXES, pairs)

    def over_core(v):
        return send(v, lambda a, b, d, e: (a, b, d, e ^ 1))

    def over_x(v):
        return send(v, lambda a, b, d, e: (a, b, d ^ 1, e))

    def over_y(v):
        return send(v, lambda a, b, d, e: (a ^ 1, b, d, e))

    def over_z(v, k):
        return send(v, lambda a, b, d, e: (a, b ^ k, d, e))

    def mids(v, k):
        return send(v, lambda a, b, d, e: (a, b ^ k, d, e), lambda a, b, d, e: b in (1, 2))

    mid = (s == 1) | (s == 2)
    normed = root_mean_square_rows(tokens.astype(F32), norm_gain).astype(BF)
    one = over_z(normed, 1)
    near = mids(normed, 3)
    tx0 = over_x(normed)
    far = mids(near, 1)
    cross = mids(one, 3)
    tx1 = over_x(one)
    last = mids(cross, 1)
    slot2 = jnp.where(mid, cross, far)
    tx2 = over_x(slot2)
    slot3 = jnp.where(mid, near, last)
    tx3 = over_x(slot3)
    early = jnp.concatenate([normed, one, slot2, tx0, tx1, tx2], axis=0)
    late = jnp.concatenate([slot3, tx3], axis=0)

    rows_w = query_diff.shape[0]
    quarter = rows_w // 4

    def pack(lo, size, head):
        parts = []
        for w in (key_diff, value_diff, query_diff, query_win):
            parts.append(lax.dynamic_slice(w, (lo, head * VDIM), (size, VDIM)))
        return jnp.concatenate(parts, axis=1)

    def kv_pack(lo, size, h):
        kv = lax.dynamic_slice(keyval_win, (nx * x + h // 2, lo, 0), (1, size, 2 * HEAD))
        return kv[0]

    def with_kv(four, kv):
        return jnp.concatenate([four[:, : 2 * VDIM], kv, four[:, 2 * VDIM :]], axis=1)

    mine_lo = (g * 2 + c) * quarter
    give_lo = (g * 2 + 1 - c) * quarter
    give = jnp.stack([pack(give_lo, quarter, 0), pack(give_lo, quarter, 1)])
    keep = jnp.stack([pack(mine_lo, quarter, 0), pack(mine_lo, quarter, 1)])
    both = jnp.concatenate([keep, over_core(give)], axis=0)
    local = pack(0, rows_w, s % 2)
    moved = send(local, lambda a, b, d, e: (a, b, d, e ^ 1), lambda a, b, d, e: e == b // 2)
    own = with_kv(jnp.where(c == s // 2, local, moved), kv_pack(0, rows_w, s))

    place = jnp.stack([s, x, c, g]).astype(jnp.int32)

    def package(k):
        h = s ^ k
        pick = lax.dynamic_index_in_dim(both, ((h // 2) ^ c) * 2 + h % 2, 0, keepdims=False)
        return pick, kv_pack(mine_lo, quarter, h)

    def chunk(part, k):
        got = over_z(part, k)
        got_y = over_y(got)
        return [got, got_y, over_core(jnp.concatenate([got, got_y], axis=0))]

    w1 = chunk(with_kv(*package(1)), 1)
    w3 = chunk(with_kv(*package(3)), 3)
    four, kv = package(2)
    w2a = chunk(jnp.concatenate([four[:, : 2 * VDIM], kv], axis=1), 2)
    w2b = chunk(four[:, 2 * VDIM :], 2)
    split = 3 * VDIM
    acc_kv, acc_q = project_early(place, early, own, w1, split)
    every = {0: ([own], 0), 1: (w1, 0), 3: (w3, 0)}
    kv_own = project_rest(place, early, late, acc_kv, every | {2: (w2a, 0)}, 0, split)
    kv_oth = over_core(kv_own)
    queries = project_rest(
        place, early, late, acc_q, every | {2: (w2b, split)}, split, own.shape[1] - split
    )

    scalars = (lam, over_core(lam), sink, over_core(sink))
    gain = output_norm_gain.reshape(1, VDIM)
    weights = [proj_diff, proj_win, over_core(proj_diff), over_core(proj_win)]

    def spread(ys):
        return [ys[0]] + [over_z(ys[k], k) for k in range(1, sp)]

    def attend(flip):
        return attention(place, scalars, gain, queries, kv_own, kv_oth, sp, nx, flip)

    far_heads = spread(attend(1))
    y_near = attend(0)
    near_heads = spread(y_near)
    received = []
    tiles = proj_diff.shape[1] // OUT_TILE
    for begin, end in ((0, tiles // 2), (tiles // 2, tiles)):
        part = output_projection(place, far_heads, weights, begin, end - begin, BF)
        received.append(over_x(part))
    kept = output_projection(place, near_heads, weights, 0, tiles, F32)
    return (kept + jnp.concatenate(received, axis=1).astype(F32)).astype(BF)


def solution(mesh):
    placed = (
        P(("grp", "sp", "tp"), None),
        P(),
        P("sp", "tp"),
        P("sp", "tp"),
        P("sp", "tp"),
        P("tp"),
        P(),
        P("sp", "tp"),
        P(None, "sp", None),
        P("tp"),
        P("tp", None),
        P("tp", None),
    )
    sizes = dict(mesh.shape)

    def body(*args):
        tokens, lam, sink = args[0], args[5], args[9]
        fits = (
            sizes["grp"] == 2
            and sizes["sp"] == 4
            and sizes["tp"] == 4
            and tokens.shape[0] == WINDOW
            and lam.shape[0] == 2
            and sink.shape[0] == 4
        )
        return (chip_body if fits else general_body)(*args)

    return jax.shard_map(
        body, mesh=mesh, in_specs=placed, out_specs=P(("grp", "sp", "tp"), None), check_vma=False
    )
```

```python
import math

import jax
import jax.numpy as jnp
from jax import lax
from jax.experimental import pallas as pl
from jax.experimental.pallas import tpu as pltpu
from jax.sharding import PartitionSpec as P


HEAD = 128
WIN_HEADS = 16
KV_HEADS = 4
WINDOW = 128
VDIM = 256
EPS = 1e-06
LOG2E = math.log2(math.e)
AXES = ("grp", "sp", "tp")

OUT_TILE = 1024
BF = jnp.bfloat16
F32 = jnp.float32


def padded_2(x, sides, width):
    for axis, dim in sides:
        devices, length = (lax.axis_size(axis), x.shape[dim])
        up = [(i, (i + 1) % devices) for i in range(devices - 1)]
        down = [(j, i) for i, j in up]
        last = lax.slice_in_dim(x, length - width, length, axis=dim)
        first = lax.slice_in_dim(x, 0, width, axis=dim)
        before = lax.ppermute(last, axis, up)
        after = lax.ppermute(first, axis, down)
        x = jnp.concatenate([before, x, after], axis=dim)
    return x


def root_mean_square_rows(values, gain):
    return values * lax.rsqrt(jnp.mean(values * values, axis=-1, keepdims=True) + EPS) * gain


def general_body(
    tokens,
    norm_gain,
    query_diff,
    key_diff,
    value_diff,
    lam,
    output_norm_gain,
    query_win,
    keyval_win,
    sink,
    proj_diff,
    proj_win,
):
    normed = root_mean_square_rows(tokens.astype(jnp.float32), norm_gain).astype(jnp.bfloat16)
    heads_diff = lam.shape[0]
    heads_win = sink.shape[0]
    group = WIN_HEADS // KV_HEADS
    kv_index = lax.axis_index("tp") * heads_win // group
    kv_local = lax.dynamic_index_in_dim(keyval_win, kv_index, 0, keepdims=False)
    pieces = [query_diff, key_diff, value_diff, query_win, kv_local]
    stacked = jnp.concatenate(pieces, axis=1)
    whole = lax.all_gather(stacked, "sp", axis=0, tiled=True)
    projected = jnp.dot(
        lax.all_gather(normed, "tp", axis=0, tiled=True), whole, preferred_element_type=jnp.float32
    )
    projected = projected.astype(jnp.bfloat16)
    output_list = []
    offset = 0
    for piece in pieces:
        output_list.append(projected[:, offset : offset + piece.shape[1]])
        offset = offset + piece.shape[1]
    q_diff, k_diff, v_diff, q_win, kv_win = output_list
    tok = projected.shape[0]
    scale = HEAD ** (-0.5)
    q_four = q_diff.reshape(tok, heads_diff, 2, HEAD)
    start_state = (
        jnp.full((heads_diff, 2, tok), -jnp.inf, jnp.float32),
        jnp.zeros((heads_diff, 2, tok), jnp.float32),
        jnp.zeros((heads_diff, 2, tok, VDIM), jnp.float32),
    )
    carry = start_state
    keys = lax.all_gather(k_diff, "sp", axis=0, tiled=True)
    values = lax.all_gather(v_diff, "sp", axis=0, tiled=True)
    rows = keys.shape[0]
    step = math.gcd(rows, 1024)
    key_blocks = keys.reshape(rows // step, step, heads_diff, 2, HEAD)
    value_blocks = values.reshape(rows // step, step, heads_diff, VDIM)

    def one(state, block):
        top, total, acc = state
        key_part, value_part = block
        scores = (
            jnp.einsum("qhmd,khmd->hmqk", q_four, key_part, preferred_element_type=jnp.float32)
            * scale
        )
        new_top = jnp.maximum(top, jnp.max(scores, axis=-1))
        expo = jnp.exp(scores - new_top[..., None])
        fade = jnp.exp(top - new_top)
        total = total * fade + jnp.sum(expo, axis=-1)
        acc = acc * fade[..., None] + jnp.einsum(
            "hmqk,khe->hmqe",
            expo.astype(jnp.bfloat16),
            value_part,
            preferred_element_type=jnp.float32,
        )
        return ((new_top, total, acc), None)

    carry, _ = lax.scan(one, carry, (key_blocks, value_blocks))
    _, total, acc = carry
    attention_maps = acc / total[..., None]
    difference_output = attention_maps[:, 0] - lam[:, None, None] * attention_maps[:, 1]
    differential_output = root_mean_square_rows(difference_output, output_norm_gain).astype(
        jnp.bfloat16
    )
    differential_output = jnp.transpose(differential_output, (1, 0, 2)).reshape(
        tok, heads_diff * VDIM
    )
    padded = padded_2(kv_win, (("sp", 0),), WINDOW)
    nblocks = tok // WINDOW
    blocks = padded.reshape(nblocks + 2, WINDOW, 2 * HEAD)
    band = jnp.concatenate([blocks[:-2], blocks[1:-1], blocks[2:]], axis=1)
    q_blocks = q_win.reshape(nblocks, WINDOW, heads_win, HEAD)
    scores = (
        jnp.einsum("nqhd,nkd->nhqk", q_blocks, band[..., :HEAD], preferred_element_type=jnp.float32)
        * scale
    )
    q_index = jnp.arange(WINDOW)
    k_index = jnp.arange(3 * WINDOW)
    relative = k_index[None, :] - WINDOW - q_index[:, None]
    first_key = lax.axis_index("sp") * tok - WINDOW
    key_pos = first_key + jnp.arange(nblocks)[:, None] * WINDOW + k_index[None, :]
    inside = (key_pos >= 0) & (key_pos < tok * lax.axis_size("sp"))
    valid = (jnp.abs(relative) <= WINDOW)[None] & inside[:, None, :]
    scores = jnp.where(valid[:, None], scores, -jnp.inf)
    sink_logit = sink[None, :, None, None]
    top_win = jnp.maximum(jnp.max(scores, axis=-1, keepdims=True), sink_logit)
    expo = jnp.exp(scores - top_win)
    weights = expo / (jnp.sum(expo, axis=-1, keepdims=True) + jnp.exp(sink_logit - top_win))
    y_win = jnp.einsum(
        "nhqk,nkd->nqhd",
        weights.astype(jnp.bfloat16),
        band[..., HEAD:],
        preferred_element_type=jnp.float32,
    ).astype(jnp.bfloat16)
    y_win = y_win.reshape(tok, heads_win * HEAD)
    summed = jnp.dot(differential_output, proj_diff, preferred_element_type=jnp.float32)
    return lax.psum_scatter(
        (summed + jnp.dot(y_win, proj_win, preferred_element_type=jnp.float32)).astype(
            jnp.bfloat16
        ),
        "tp",
        scatter_dimension=0,
        tiled=True,
    )


def row_of(i, s, x, nx, rows):
    slot = (i // nx) ^ s
    side = (i % nx) ^ x
    early = rows // WINDOW // nx - 1
    row = jnp.where(slot < early, side * early + slot, nx * early + side) * WINDOW
    return pl.multiple_of(row, WINDOW)


def attention_kernel(
    place, lam_a, lam_b, sink_a, sink_b, gain, q_ref, own_ref, oth_ref, *outs, nx, flip
):
    step = pl.program_id(0)
    s, x, c = place[0], place[1], place[2]
    rows = own_ref.shape[0]
    blocks = 2
    scale = HEAD**-0.5
    swapped = ((s // 2) ^ c) == 1
    lam = jnp.where(swapped, lam_b[s % 2], lam_a[s % 2])
    sinks = [
        jnp.where(swapped, sink_b[(s % 2) * 2 + h], sink_a[(s % 2) * 2 + h]) for h in range(2)
    ]
    nt = (((1,), (1,)), ((), ()))
    at = [((step * blocks + j) ^ s) * nx + (x ^ flip) for j in range(blocks)]
    places = [row_of(i, s, x, nx, rows) for i in at]

    def q_of(lanes):
        return jnp.concatenate([q_ref[pl.ds(r, WINDOW), lanes] for r in places], axis=0)

    maps = []
    for m in range(2):
        lanes = slice(m * HEAD, (m + 1) * HEAD)
        q = q_of(lanes)
        sa = lax.dot_general(q, own_ref[:, lanes], nt, preferred_element_type=F32)
        sb = lax.dot_general(q, oth_ref[:, lanes], nt, preferred_element_type=F32)
        top = jnp.maximum(
            jnp.max(sa, axis=-1, keepdims=True), jnp.max(sb, axis=-1, keepdims=True)
        )
        top = top * (scale * LOG2E)
        ea = jnp.exp2(sa * (scale * LOG2E) - top)
        eb = jnp.exp2(sb * (scale * LOG2E) - top)
        total = jnp.sum(ea, axis=-1, keepdims=True) + jnp.sum(eb, axis=-1, keepdims=True)
        acc = jnp.dot(ea.astype(BF), own_ref[:, 256:512], preferred_element_type=F32)
        acc = acc + jnp.dot(eb.astype(BF), oth_ref[:, 256:512], preferred_element_type=F32)
        maps.append(acc / total)
    d = maps[0] - lam * maps[1]
    y = d * lax.rsqrt(jnp.mean(d * d, axis=-1, keepdims=True) + EPS) * gain[...]
    y = y.astype(BF)
    last = rows // WINDOW - 1
    kw = slice(512, 512 + HEAD)
    vw = slice(512 + HEAD, 512 + 2 * HEAD)
    q_at = lax.broadcasted_iota(jnp.int32, (WINDOW, WINDOW), 0)
    k_at = lax.broadcasted_iota(jnp.int32, (WINDOW, WINDOW), 1)
    wins = []
    for i, r_own in zip(at, places):
        before = i - 1 + c
        after = i + c
        r_bef = row_of(jnp.maximum(before, 0), s, x, nx, rows)
        r_aft = row_of(jnp.minimum(after, last), s, x, nx, rows)
        k0 = oth_ref[pl.ds(r_bef, WINDOW), kw]
        k1 = own_ref[pl.ds(r_own, WINDOW), kw]
        k2 = oth_ref[pl.ds(r_aft, WINDOW), kw]
        v0 = oth_ref[pl.ds(r_bef, WINDOW), vw]
        v1 = own_ref[pl.ds(r_own, WINDOW), vw]
        v2 = oth_ref[pl.ds(r_aft, WINDOW), vw]
        ok0 = (k_at >= q_at) & (before >= 0)
        ok2 = (k_at <= q_at) & (after <= last)
        for h in range(2):
            q = q_ref[pl.ds(r_own, WINDOW), 256 + h * HEAD : 256 + (h + 1) * HEAD]
            z0 = lax.dot_general(q, k0, nt, preferred_element_type=F32) * scale
            z1 = lax.dot_general(q, k1, nt, preferred_element_type=F32) * scale
            z2 = lax.dot_general(q, k2, nt, preferred_element_type=F32) * scale
            z0 = jnp.where(ok0, z0, -jnp.inf)
            z2 = jnp.where(ok2, z2, -jnp.inf)
            top = jnp.max(jnp.maximum(jnp.maximum(z0, z1), z2), axis=-1, keepdims=True)
            top = jnp.maximum(top, sinks[h])
            e0, e1, e2 = jnp.exp(z0 - top), jnp.exp(z1 - top), jnp.exp(z2 - top)
            total = jnp.sum(e0 + e1 + e2, axis=-1, keepdims=True) + jnp.exp(sinks[h] - top)
            w = 1.0 / total
            acc = jnp.dot((e0 * w).astype(BF), v0, preferred_element_type=F32)
            acc = acc + jnp.dot((e1 * w).astype(BF), v1, preferred_element_type=F32)
            acc = acc + jnp.dot((e2 * w).astype(BF), v2, preferred_element_type=F32)
            wins.append(acc.astype(BF))
    for t in range(len(outs) // blocks):

        @pl.when(step == t)
        def _(t=t):
            for j in range(blocks):
                out = outs[t * blocks + j]
                out[:, 0:VDIM] = y[j * WINDOW : (j + 1) * WINDOW]
                out[:, VDIM : VDIM + HEAD] = wins[2 * j]
                out[:, VDIM + HEAD : VDIM + 2 * HEAD] = wins[2 * j + 1]


def attention(place, scalars, gain, q, own, oth, sp, nx, flip):
    rows = own.shape[0]
    smem = pl.BlockSpec(memory_space=pltpu.SMEM)
    whole = pl.BlockSpec(own.shape, lambda i: (0, 0))
    block = pl.BlockSpec((WINDOW, 2 * VDIM), lambda i: (0, 0))

    def kernel(*refs):
        attention_kernel(*refs, nx=nx, flip=flip)

    return pl.pallas_call(
        kernel,
        grid=(sp // 2,),
        in_specs=[smem] * 5
        + [pl.BlockSpec((1, VDIM), lambda i: (0, 0)), pl.BlockSpec(q.shape, lambda i: (0, 0))]
        + [whole, whole],
        out_specs=[block] * sp,
        out_shape=[jax.ShapeDtypeStruct((WINDOW, 2 * VDIM), BF)] * sp,
        compiler_params=pltpu.CompilerParams(
            dimension_semantics=("arbitrary",), vmem_limit_bytes=20 * 2**20
        ),
        cost_estimate=pl.CostEstimate(
            flops=4 * sp * WINDOW * rows * 2 * 384,
            bytes_accessed=4 * 2**20,
            transcendentals=0,
        ),
        name="attend",
    )(place, *scalars, gain, q, own, oth)


def assemble(scratch, row, pieces, g, c):
    size = pieces[0].shape[0]
    parts = []
    for p in pieces:
        for lo in range(0, p.shape[0], size):
            parts.append(p[lo : lo + size, :])
    if len(parts) == 1:
        scratch[row : row + size, :] = parts[0]
        return
    for j, part in enumerate(parts):
        quarter = (g ^ (j & 1)) * 2 + (c ^ (j >> 1))
        scratch[pl.ds(pl.multiple_of(row + quarter * size, size), size), :] = part


ROWS = 256


def project_sum(place, acts, sums, chunks, split):
    rows = acts.shape[0]
    cols = chunks[0][1][0].shape[1]
    wide = sum(p.shape[0] for p in chunks[0][1])
    widths = (split, cols - split)

    def kernel(place_ref, *refs):
        (*refs, left, right, scratch) = refs
        before = (refs.pop(0), refs.pop(0)) if sums else None
        parts = []
        for _, pieces in chunks:
            a, ws = refs[0], refs[1 : 1 + len(pieces)]
            refs = refs[1 + len(pieces) :]
            parts.append((a, ws))

        @pl.when(pl.program_id(0) == 0)
        def _():
            for _, ws in parts:
                if len(ws) > 1:
                    assemble(scratch, 0, ws, place_ref[3], place_ref[2])

        total = None
        for a, ws in parts:
            w = scratch[...] if len(ws) > 1 else ws[0][...]
            part = jnp.dot(a[...], w, preferred_element_type=F32)
            total = part if total is None else total + part
        for out, lo, hi, j in ((left, 0, split, 0), (right, split, cols, 1)):
            out[...] = total[:, lo:hi] + before[j][...] if before else total[:, lo:hi]

    in_specs, operands = [], []
    if sums:
        in_specs += [pl.BlockSpec((ROWS, w), lambda m, at: (m, 0)) for w in widths]
        operands += sums
    for k, pieces in chunks:
        in_specs.append(pl.BlockSpec((ROWS, wide), lambda m, at, k=k: (m, at[0] ^ k)))
        in_specs += [pl.BlockSpec(p.shape, lambda m, at: (0, 0)) for p in pieces]
        operands += [acts, *pieces]
    return pl.pallas_call(
        kernel,
        grid_spec=pltpu.PrefetchScalarGridSpec(
            num_scalar_prefetch=1,
            grid=(rows // ROWS,),
            in_specs=in_specs,
            out_specs=[pl.BlockSpec((ROWS, w), lambda m, at: (m, 0)) for w in widths],
            scratch_shapes=[pltpu.VMEM((wide, cols), BF)],
        ),
        out_shape=[jax.ShapeDtypeStruct((rows, w), F32) for w in widths],
        compiler_params=pltpu.CompilerParams(
            dimension_semantics=("arbitrary",), vmem_limit_bytes=26 * 2**20
        ),
        cost_estimate=pl.CostEstimate(
            flops=2 * rows * wide * cols * len(chunks),
            bytes_accessed=rows * cols * 4,
            transcendentals=0,
        ),
        name="project",
    )(place, *operands)


def project_rest(place, early, late, acc_early, acc_late, third, second, begin):
    rows, cols = acc_early.shape
    wide = sum(p.shape[0] for p in third)
    steps = rows // ROWS

    def kernel(place_ref, acc_e, acc_l, e2, l2, l3, *refs):
        (*ws, out, scratch) = refs
        m = pl.program_id(0)

        @pl.when(m == 0)
        def _():
            n = len(second)
            assemble(scratch, 0, ws[:n], place_ref[3], place_ref[2])
            assemble(scratch, wide, ws[n:], place_ref[3], place_ref[2])

        def part(a, j):
            return jnp.dot(
                a[...], scratch[j * wide : (j + 1) * wide], preferred_element_type=F32
            )

        @pl.when(m < steps)
        def _():
            out[...] = (acc_e[...] + part(e2, 0)).astype(BF)

        @pl.when(m == steps)
        def _():
            out[...] = (acc_l[...] + part(l2, 0) + part(l3, 1)).astype(BF)

    def clamped(m):
        return jnp.minimum(m, steps - 1)

    in_specs = [
        pl.BlockSpec((ROWS, cols), lambda m, at: (clamped(m), 0)),
        pl.BlockSpec((ROWS, cols), lambda m, at: (0, 0)),
        pl.BlockSpec((ROWS, wide), lambda m, at: (clamped(m), at[0] ^ 2)),
        pl.BlockSpec((ROWS, wide), lambda m, at: (0, at[0] ^ 2)),
        pl.BlockSpec((ROWS, wide), lambda m, at: (0, at[0] ^ 3)),
    ]
    in_specs += [pl.BlockSpec(p.shape, lambda m, at: (0, 0)) for p in second]
    in_specs += [
        pl.BlockSpec((pl.Element(p.shape[0]), pl.Element(cols)), lambda m, at: (0, begin))
        for p in third
    ]
    return pl.pallas_call(
        kernel,
        grid_spec=pltpu.PrefetchScalarGridSpec(
            num_scalar_prefetch=1,
            grid=(steps + 1,),
            in_specs=in_specs,
            out_specs=pl.BlockSpec((ROWS, cols), lambda m, at: (m, 0)),
            scratch_shapes=[pltpu.VMEM((2 * wide, cols), BF)],
        ),
        out_shape=jax.ShapeDtypeStruct((rows + late.shape[0], cols), BF),
        compiler_params=pltpu.CompilerParams(
            dimension_semantics=("arbitrary",), vmem_limit_bytes=26 * 2**20
        ),
        cost_estimate=pl.CostEstimate(
            flops=3 * (rows + late.shape[0]) * wide * cols,
            bytes_accessed=8 * 2**20,
            transcendentals=0,
        ),
        name="project",
    )(place, acc_early, acc_late, early, late, late, *second, *third)


def output_projection(place, heads, weights, first, count, kind):
    sp = len(heads)
    tile = OUT_TILE

    def kernel(place_ref, *refs):
        ys, ws, (out, ordered) = refs[:sp], refs[sp : sp + 4], refs[sp + 4 :]
        s, c = place_ref[0], place_ref[2]
        n = pl.program_id(0)

        @pl.when(n == 0)
        def _():
            for k, y in enumerate(ys):
                ordered[(s ^ k) ^ (2 * c)] = y[...]

        total = None
        for j, w in enumerate(ws):
            lanes = slice((j % 2) * VDIM, (j % 2 + 1) * VDIM)
            for local in range(2):
                part = jnp.dot(
                    ordered[(j // 2) * 2 + local, :, lanes],
                    w[local * VDIM : (local + 1) * VDIM],
                    preferred_element_type=F32,
                )
                total = part if total is None else total + part
        out[...] = total.astype(out.dtype)

    whole = pl.BlockSpec((WINDOW, 2 * VDIM), lambda n: (0, 0))
    in_specs = [pl.BlockSpec(memory_space=pltpu.SMEM)] + [whole] * sp
    in_specs += [pl.BlockSpec((2 * VDIM, tile), lambda n: (0, n + first))] * 4
    operands = [place, *heads, *weights]
    return pl.pallas_call(
        kernel,
        grid=(count,),
        in_specs=in_specs,
        out_specs=pl.BlockSpec((WINDOW, tile), lambda n: (0, n)),
        out_shape=jax.ShapeDtypeStruct((WINDOW, count * tile), kind),
        scratch_shapes=[pltpu.VMEM((sp, WINDOW, 2 * VDIM), BF)],
        compiler_params=pltpu.CompilerParams(
            dimension_semantics=("arbitrary",), vmem_limit_bytes=16 * 2**20
        ),
        cost_estimate=pl.CostEstimate(
            flops=2 * WINDOW * 2048 * count * tile,
            bytes_accessed=2048 * count * tile * 2,
            transcendentals=0,
        ),
        name="output",
    )(*operands)


def chip_body(
    tokens,
    norm_gain,
    query_diff,
    key_diff,
    value_diff,
    lam,
    output_norm_gain,
    query_win,
    keyval_win,
    sink,
    proj_diff,
    proj_win,
):
    ng, sp, tp = (lax.axis_size(a) for a in AXES)
    nx = tp // 2
    g, s, t = (lax.axis_index(a) for a in AXES)
    x, c = t // 2, t % 2

    def send(value, target, only=None):
        pairs = []
        for i in range(ng * sp * tp):
            at = (i // (sp * tp), i // tp % sp, i % tp // 2, i % 2)
            if only is None or only(*at):
                a, b, d, e = target(*at)
                pairs.append((i, ((a * sp + b) * nx + d) * 2 + e))
        return lax.ppermute(value, AXES, pairs)

    def over_core(v):
        return send(v, lambda a, b, d, e: (a, b, d, e ^ 1))

    def over_x(v):
        return send(v, lambda a, b, d, e: (a, b, d ^ 1, e))

    def over_y(v):
        return send(v, lambda a, b, d, e: (a ^ 1, b, d, e))

    def over_z(v, k):
        return send(v, lambda a, b, d, e: (a, b ^ k, d, e))

    def mids(v, k):
        return send(v, lambda a, b, d, e: (a, b ^ k, d, e), lambda a, b, d, e: b in (1, 2))

    mid = (s == 1) | (s == 2)
    normed = root_mean_square_rows(tokens.astype(F32), norm_gain).astype(BF)
    one = over_z(normed, 1)
    near = mids(normed, 3)
    tx0 = over_x(normed)
    far = mids(near, 1)
    cross = mids(one, 3)
    tx1 = over_x(one)
    last = mids(cross, 1)
    slot2 = jnp.where(mid, cross, far)
    tx2 = over_x(slot2)
    slot3 = jnp.where(mid, near, last)
    tx3 = over_x(slot3)
    early = jnp.concatenate([normed, one, slot2, tx0, tx1, tx2], axis=0)
    late = jnp.concatenate([slot3, tx3], axis=0)

    rows_w = query_diff.shape[0]
    quarter = rows_w // 4

    def pack(lo, size, head):
        parts = []
        for w in (key_diff, value_diff, query_diff, query_win):
            parts.append(lax.dynamic_slice(w, (lo, head * VDIM), (size, VDIM)))
        return jnp.concatenate(parts, axis=1)

    def kv_pack(lo, size, h):
        kv = lax.dynamic_slice(keyval_win, (nx * x + h // 2, lo, 0), (1, size, 2 * HEAD))
        return kv[0]

    def with_kv(four, kv):
        return jnp.concatenate([four[:, : 2 * VDIM], kv, four[:, 2 * VDIM :]], axis=1)

    mine_lo = (g * 2 + c) * quarter
    give_lo = (g * 2 + 1 - c) * quarter
    give = jnp.stack([pack(give_lo, quarter, 0), pack(give_lo, quarter, 1)])
    keep = jnp.stack([pack(mine_lo, quarter, 0), pack(mine_lo, quarter, 1)])
    both = jnp.concatenate([keep, over_core(give)], axis=0)
    local = pack(0, rows_w, s % 2)
    moved = send(local, lambda a, b, d, e: (a, b, d, e ^ 1), lambda a, b, d, e: e == b // 2)
    own = with_kv(jnp.where(c == s // 2, local, moved), kv_pack(0, rows_w, s))

    place = jnp.stack([s, x, c, g]).astype(jnp.int32)

    def package(k):
        h = s ^ k
        pick = lax.dynamic_index_in_dim(both, ((h // 2) ^ c) * 2 + h % 2, 0, keepdims=False)
        return pick, kv_pack(mine_lo, quarter, h)

    def chunk(part, k):
        got = over_z(part, k)
        got_y = over_y(got)
        return [got, got_y, over_core(jnp.concatenate([got, got_y], axis=0))]

    w1 = chunk(with_kv(*package(1)), 1)
    w3 = chunk(with_kv(*package(3)), 3)
    four, kv = package(2)
    w2a = chunk(jnp.concatenate([four[:, : 2 * VDIM], kv], axis=1), 2)
    w2b = chunk(four[:, 2 * VDIM :], 2)
    split = 3 * VDIM
    first = [(0, [own]), (1, w1)]
    sums = project_sum(place, early, None, first, split)
    ends = project_sum(place, late, None, first, split)
    sums = project_sum(place, early, sums, [(3, w3)], split)
    kv_own = project_rest(place, early, late, sums[0], ends[0], w3, w2a, 0)
    kv_oth = over_core(kv_own)
    queries = project_rest(place, early, late, sums[1], ends[1], w3, w2b, split)

    scalars = (lam, over_core(lam), sink, over_core(sink))
    gain = output_norm_gain.reshape(1, VDIM)
    weights = [proj_diff, proj_win, over_core(proj_diff), over_core(proj_win)]

    def spread(ys):
        return [ys[0]] + [over_z(ys[k], k) for k in range(1, sp)]

    def attend(flip):
        return attention(place, scalars, gain, queries, kv_own, kv_oth, sp, nx, flip)

    far_heads = spread(attend(1))
    y_near = attend(0)
    near_heads = spread(y_near)
    received = []
    tiles = proj_diff.shape[1] // OUT_TILE
    for begin, end in ((0, tiles // 2), (tiles // 2, tiles)):
        part = output_projection(place, far_heads, weights, begin, end - begin, BF)
        received.append(over_x(part))
    kept = output_projection(place, near_heads, weights, 0, tiles, F32)
    return (kept + jnp.concatenate(received, axis=1).astype(F32)).astype(BF)


def solution(mesh):
    placed = (
        P(("grp", "sp", "tp"), None),
        P(),
        P("sp", "tp"),
        P("sp", "tp"),
        P("sp", "tp"),
        P("tp"),
        P(),
        P("sp", "tp"),
        P(None, "sp", None),
        P("tp"),
        P("tp", None),
        P("tp", None),
    )
    sizes = dict(mesh.shape)

    def body(*args):
        tokens, lam, sink = args[0], args[5], args[9]
        fits = (
            sizes["grp"] == 2
            and sizes["sp"] == 4
            and sizes["tp"] == 4
            and tokens.shape[0] == WINDOW
            and lam.shape[0] == 2
            and sink.shape[0] == 4
        )
        return (chip_body if fits else general_body)(*args)

    return jax.shard_map(
        body, mesh=mesh, in_specs=placed, out_specs=P(("grp", "sp", "tp"), None), check_vma=False
    )
```

```python
import math

import jax
import jax.numpy as jnp
from jax import lax
from jax.experimental import pallas as pl
from jax.experimental.pallas import tpu as pltpu
from jax.sharding import PartitionSpec as P


HEAD = 128
WIN_HEADS = 16
KV_HEADS = 4
WINDOW = 128
VDIM = 256
EPS = 1e-06
LOG2E = math.log2(math.e)
AXES = ("grp", "sp", "tp")

OUT_TILE = 1024
BF = jnp.bfloat16
F32 = jnp.float32


def padded_2(x, sides, width):
    for axis, dim in sides:
        devices, length = (lax.axis_size(axis), x.shape[dim])
        up = [(i, (i + 1) % devices) for i in range(devices - 1)]
        down = [(j, i) for i, j in up]
        last = lax.slice_in_dim(x, length - width, length, axis=dim)
        first = lax.slice_in_dim(x, 0, width, axis=dim)
        before = lax.ppermute(last, axis, up)
        after = lax.ppermute(first, axis, down)
        x = jnp.concatenate([before, x, after], axis=dim)
    return x


def root_mean_square_rows(values, gain):
    return values * lax.rsqrt(jnp.mean(values * values, axis=-1, keepdims=True) + EPS) * gain


def general_body(
    tokens,
    norm_gain,
    query_diff,
    key_diff,
    value_diff,
    lam,
    output_norm_gain,
    query_win,
    keyval_win,
    sink,
    proj_diff,
    proj_win,
):
    normed = root_mean_square_rows(tokens.astype(jnp.float32), norm_gain).astype(jnp.bfloat16)
    heads_diff = lam.shape[0]
    heads_win = sink.shape[0]
    group = WIN_HEADS // KV_HEADS
    kv_index = lax.axis_index("tp") * heads_win // group
    kv_local = lax.dynamic_index_in_dim(keyval_win, kv_index, 0, keepdims=False)
    pieces = [query_diff, key_diff, value_diff, query_win, kv_local]
    stacked = jnp.concatenate(pieces, axis=1)
    whole = lax.all_gather(stacked, "sp", axis=0, tiled=True)
    projected = jnp.dot(
        lax.all_gather(normed, "tp", axis=0, tiled=True), whole, preferred_element_type=jnp.float32
    )
    projected = projected.astype(jnp.bfloat16)
    output_list = []
    offset = 0
    for piece in pieces:
        output_list.append(projected[:, offset : offset + piece.shape[1]])
        offset = offset + piece.shape[1]
    q_diff, k_diff, v_diff, q_win, kv_win = output_list
    tok = projected.shape[0]
    scale = HEAD ** (-0.5)
    q_four = q_diff.reshape(tok, heads_diff, 2, HEAD)
    start_state = (
        jnp.full((heads_diff, 2, tok), -jnp.inf, jnp.float32),
        jnp.zeros((heads_diff, 2, tok), jnp.float32),
        jnp.zeros((heads_diff, 2, tok, VDIM), jnp.float32),
    )
    carry = start_state
    keys = lax.all_gather(k_diff, "sp", axis=0, tiled=True)
    values = lax.all_gather(v_diff, "sp", axis=0, tiled=True)
    rows = keys.shape[0]
    step = math.gcd(rows, 1024)
    key_blocks = keys.reshape(rows // step, step, heads_diff, 2, HEAD)
    value_blocks = values.reshape(rows // step, step, heads_diff, VDIM)

    def one(state, block):
        top, total, acc = state
        key_part, value_part = block
        scores = (
            jnp.einsum("qhmd,khmd->hmqk", q_four, key_part, preferred_element_type=jnp.float32)
            * scale
        )
        new_top = jnp.maximum(top, jnp.max(scores, axis=-1))
        expo = jnp.exp(scores - new_top[..., None])
        fade = jnp.exp(top - new_top)
        total = total * fade + jnp.sum(expo, axis=-1)
        acc = acc * fade[..., None] + jnp.einsum(
            "hmqk,khe->hmqe",
            expo.astype(jnp.bfloat16),
            value_part,
            preferred_element_type=jnp.float32,
        )
        return ((new_top, total, acc), None)

    carry, _ = lax.scan(one, carry, (key_blocks, value_blocks))
    _, total, acc = carry
    attention_maps = acc / total[..., None]
    difference_output = attention_maps[:, 0] - lam[:, None, None] * attention_maps[:, 1]
    differential_output = root_mean_square_rows(difference_output, output_norm_gain).astype(
        jnp.bfloat16
    )
    differential_output = jnp.transpose(differential_output, (1, 0, 2)).reshape(
        tok, heads_diff * VDIM
    )
    padded = padded_2(kv_win, (("sp", 0),), WINDOW)
    nblocks = tok // WINDOW
    blocks = padded.reshape(nblocks + 2, WINDOW, 2 * HEAD)
    band = jnp.concatenate([blocks[:-2], blocks[1:-1], blocks[2:]], axis=1)
    q_blocks = q_win.reshape(nblocks, WINDOW, heads_win, HEAD)
    scores = (
        jnp.einsum("nqhd,nkd->nhqk", q_blocks, band[..., :HEAD], preferred_element_type=jnp.float32)
        * scale
    )
    q_index = jnp.arange(WINDOW)
    k_index = jnp.arange(3 * WINDOW)
    relative = k_index[None, :] - WINDOW - q_index[:, None]
    first_key = lax.axis_index("sp") * tok - WINDOW
    key_pos = first_key + jnp.arange(nblocks)[:, None] * WINDOW + k_index[None, :]
    inside = (key_pos >= 0) & (key_pos < tok * lax.axis_size("sp"))
    valid = (jnp.abs(relative) <= WINDOW)[None] & inside[:, None, :]
    scores = jnp.where(valid[:, None], scores, -jnp.inf)
    sink_logit = sink[None, :, None, None]
    top_win = jnp.maximum(jnp.max(scores, axis=-1, keepdims=True), sink_logit)
    expo = jnp.exp(scores - top_win)
    weights = expo / (jnp.sum(expo, axis=-1, keepdims=True) + jnp.exp(sink_logit - top_win))
    y_win = jnp.einsum(
        "nhqk,nkd->nqhd",
        weights.astype(jnp.bfloat16),
        band[..., HEAD:],
        preferred_element_type=jnp.float32,
    ).astype(jnp.bfloat16)
    y_win = y_win.reshape(tok, heads_win * HEAD)
    summed = jnp.dot(differential_output, proj_diff, preferred_element_type=jnp.float32)
    return lax.psum_scatter(
        (summed + jnp.dot(y_win, proj_win, preferred_element_type=jnp.float32)).astype(
            jnp.bfloat16
        ),
        "tp",
        scatter_dimension=0,
        tiled=True,
    )


def row_of(i, s, x, nx, rows):
    slot = (i // nx) ^ s
    side = (i % nx) ^ x
    early = rows // WINDOW // nx - 1
    row = jnp.where(slot < early, side * early + slot, nx * early + side) * WINDOW
    return pl.multiple_of(row, WINDOW)


def attention_kernel(
    place, lam_a, lam_b, sink_a, sink_b, gain, q_ref, own_ref, oth_ref, *outs, nx, flip, first
):
    step = pl.program_id(0)
    s, x, c = place[0], place[1], place[2]
    rows = own_ref.shape[0]
    blocks = 2
    scale = HEAD**-0.5
    swapped = ((s // 2) ^ c) == 1
    lam = jnp.where(swapped, lam_b[s % 2], lam_a[s % 2])
    sinks = [
        jnp.where(swapped, sink_b[(s % 2) * 2 + h], sink_a[(s % 2) * 2 + h]) for h in range(2)
    ]
    nt = (((1,), (1,)), ((), ()))
    at = [((step * blocks + j + first) ^ s) * nx + (x ^ flip) for j in range(blocks)]
    places = [row_of(i, s, x, nx, rows) for i in at]

    def q_of(lanes):
        return jnp.concatenate([q_ref[pl.ds(r, WINDOW), lanes] for r in places], axis=0)

    maps = []
    for m in range(2):
        lanes = slice(m * HEAD, (m + 1) * HEAD)
        q = q_of(lanes)
        sa = lax.dot_general(q, own_ref[:, lanes], nt, preferred_element_type=F32)
        sb = lax.dot_general(q, oth_ref[:, lanes], nt, preferred_element_type=F32)
        top = jnp.maximum(
            jnp.max(sa, axis=-1, keepdims=True), jnp.max(sb, axis=-1, keepdims=True)
        )
        top = top * (scale * LOG2E)
        ea = jnp.exp2(sa * (scale * LOG2E) - top)
        eb = jnp.exp2(sb * (scale * LOG2E) - top)
        total = jnp.sum(ea, axis=-1, keepdims=True) + jnp.sum(eb, axis=-1, keepdims=True)
        acc = jnp.dot(ea.astype(BF), own_ref[:, 256:512], preferred_element_type=F32)
        acc = acc + jnp.dot(eb.astype(BF), oth_ref[:, 256:512], preferred_element_type=F32)
        maps.append(acc / total)
    d = maps[0] - lam * maps[1]
    y = d * lax.rsqrt(jnp.mean(d * d, axis=-1, keepdims=True) + EPS) * gain[...]
    y = y.astype(BF)
    last = rows // WINDOW - 1
    kw = slice(512, 512 + HEAD)
    vw = slice(512 + HEAD, 512 + 2 * HEAD)
    q_at = lax.broadcasted_iota(jnp.int32, (WINDOW, WINDOW), 0)
    k_at = lax.broadcasted_iota(jnp.int32, (WINDOW, WINDOW), 1)
    wins = []
    for i, r_own in zip(at, places):
        before = i - 1 + c
        after = i + c
        r_bef = row_of(jnp.maximum(before, 0), s, x, nx, rows)
        r_aft = row_of(jnp.minimum(after, last), s, x, nx, rows)
        k0 = oth_ref[pl.ds(r_bef, WINDOW), kw]
        k1 = own_ref[pl.ds(r_own, WINDOW), kw]
        k2 = oth_ref[pl.ds(r_aft, WINDOW), kw]
        v0 = oth_ref[pl.ds(r_bef, WINDOW), vw]
        v1 = own_ref[pl.ds(r_own, WINDOW), vw]
        v2 = oth_ref[pl.ds(r_aft, WINDOW), vw]
        ok0 = (k_at >= q_at) & (before >= 0)
        ok2 = (k_at <= q_at) & (after <= last)
        for h in range(2):
            q = q_ref[pl.ds(r_own, WINDOW), 256 + h * HEAD : 256 + (h + 1) * HEAD]
            z0 = lax.dot_general(q, k0, nt, preferred_element_type=F32) * scale
            z1 = lax.dot_general(q, k1, nt, preferred_element_type=F32) * scale
            z2 = lax.dot_general(q, k2, nt, preferred_element_type=F32) * scale
            z0 = jnp.where(ok0, z0, -jnp.inf)
            z2 = jnp.where(ok2, z2, -jnp.inf)
            top = jnp.max(jnp.maximum(jnp.maximum(z0, z1), z2), axis=-1, keepdims=True)
            top = jnp.maximum(top, sinks[h])
            e0, e1, e2 = jnp.exp(z0 - top), jnp.exp(z1 - top), jnp.exp(z2 - top)
            total = jnp.sum(e0 + e1 + e2, axis=-1, keepdims=True) + jnp.exp(sinks[h] - top)
            w = 1.0 / total
            acc = jnp.dot((e0 * w).astype(BF), v0, preferred_element_type=F32)
            acc = acc + jnp.dot((e1 * w).astype(BF), v1, preferred_element_type=F32)
            acc = acc + jnp.dot((e2 * w).astype(BF), v2, preferred_element_type=F32)
            wins.append(acc.astype(BF))
    for t in range(len(outs) // blocks):

        @pl.when(step == t)
        def _(t=t):
            for j in range(blocks):
                out = outs[t * blocks + j]
                out[:, 0:VDIM] = y[j * WINDOW : (j + 1) * WINDOW]
                out[:, VDIM : VDIM + HEAD] = wins[2 * j]
                out[:, VDIM + HEAD : VDIM + 2 * HEAD] = wins[2 * j + 1]


def attention(place, scalars, gain, q, own, oth, nx, flip, first, count):
    rows = own.shape[0]
    smem = pl.BlockSpec(memory_space=pltpu.SMEM)
    whole = pl.BlockSpec(own.shape, lambda i: (0, 0))
    block = pl.BlockSpec((WINDOW, 2 * VDIM), lambda i: (0, 0))

    def kernel(*refs):
        attention_kernel(*refs, nx=nx, flip=flip, first=first)

    return pl.pallas_call(
        kernel,
        grid=(count // 2,),
        in_specs=[smem] * 5
        + [pl.BlockSpec((1, VDIM), lambda i: (0, 0)), pl.BlockSpec(q.shape, lambda i: (0, 0))]
        + [whole, whole],
        out_specs=[block] * count,
        out_shape=[jax.ShapeDtypeStruct((WINDOW, 2 * VDIM), BF)] * count,
        compiler_params=pltpu.CompilerParams(
            dimension_semantics=("arbitrary",), vmem_limit_bytes=20 * 2**20
        ),
        cost_estimate=pl.CostEstimate(
            flops=4 * count * WINDOW * rows * 2 * 384,
            bytes_accessed=4 * 2**20,
            transcendentals=0,
        ),
        name="attend",
    )(place, *scalars, gain, q, own, oth)


def assemble(scratch, row, pieces, g, c):
    size = pieces[0].shape[0]
    parts = []
    for p in pieces:
        for lo in range(0, p.shape[0], size):
            parts.append(p[lo : lo + size, :])
    if len(parts) == 1:
        scratch[row : row + size, :] = parts[0]
        return
    for j, part in enumerate(parts):
        quarter = (g ^ (j & 1)) * 2 + (c ^ (j >> 1))
        scratch[pl.ds(pl.multiple_of(row + quarter * size, size), size), :] = part


ROWS = 256


def project_sum(place, acts, sums, chunks, split):
    rows = acts.shape[0]
    cols = chunks[0][1][0].shape[1]
    wide = sum(p.shape[0] for p in chunks[0][1])
    widths = (split, cols - split)

    def kernel(place_ref, *refs):
        (*refs, left, right, scratch) = refs
        before = (refs.pop(0), refs.pop(0)) if sums else None
        parts = []
        for _, pieces in chunks:
            a, ws = refs[0], refs[1 : 1 + len(pieces)]
            refs = refs[1 + len(pieces) :]
            parts.append((a, ws))

        @pl.when(pl.program_id(0) == 0)
        def _():
            for _, ws in parts:
                if len(ws) > 1:
                    assemble(scratch, 0, ws, place_ref[3], place_ref[2])

        total = None
        for a, ws in parts:
            w = scratch[...] if len(ws) > 1 else ws[0][...]
            part = jnp.dot(a[...], w, preferred_element_type=F32)
            total = part if total is None else total + part
        for out, lo, hi, j in ((left, 0, split, 0), (right, split, cols, 1)):
            out[...] = total[:, lo:hi] + before[j][...] if before else total[:, lo:hi]

    in_specs, operands = [], []
    if sums:
        in_specs += [pl.BlockSpec((ROWS, w), lambda m, at: (m, 0)) for w in widths]
        operands += sums
    for k, pieces in chunks:
        in_specs.append(pl.BlockSpec((ROWS, wide), lambda m, at, k=k: (m, at[0] ^ k)))
        in_specs += [pl.BlockSpec(p.shape, lambda m, at: (0, 0)) for p in pieces]
        operands += [acts, *pieces]
    return pl.pallas_call(
        kernel,
        grid_spec=pltpu.PrefetchScalarGridSpec(
            num_scalar_prefetch=1,
            grid=(rows // ROWS,),
            in_specs=in_specs,
            out_specs=[pl.BlockSpec((ROWS, w), lambda m, at: (m, 0)) for w in widths],
            scratch_shapes=[pltpu.VMEM((wide, cols), BF)],
        ),
        out_shape=[jax.ShapeDtypeStruct((rows, w), F32) for w in widths],
        compiler_params=pltpu.CompilerParams(
            dimension_semantics=("arbitrary",), vmem_limit_bytes=26 * 2**20
        ),
        cost_estimate=pl.CostEstimate(
            flops=2 * rows * wide * cols * len(chunks),
            bytes_accessed=rows * cols * 4,
            transcendentals=0,
        ),
        name="project",
    )(place, *operands)


def project_rest(place, early, late, acc_early, acc_late, third, second, begin):
    rows, cols = acc_early.shape
    wide = sum(p.shape[0] for p in third)
    steps = rows // ROWS

    def kernel(place_ref, acc_e, acc_l, e2, l2, l3, *refs):
        (*ws, out, scratch) = refs
        m = pl.program_id(0)

        @pl.when(m == 0)
        def _():
            n = len(second)
            assemble(scratch, 0, ws[:n], place_ref[3], place_ref[2])
            assemble(scratch, wide, ws[n:], place_ref[3], place_ref[2])

        def part(a, j):
            return jnp.dot(
                a[...], scratch[j * wide : (j + 1) * wide], preferred_element_type=F32
            )

        @pl.when(m < steps)
        def _():
            out[...] = (acc_e[...] + part(e2, 0)).astype(BF)

        @pl.when(m == steps)
        def _():
            out[...] = (acc_l[...] + part(l2, 0) + part(l3, 1)).astype(BF)

    def clamped(m):
        return jnp.minimum(m, steps - 1)

    in_specs = [
        pl.BlockSpec((ROWS, cols), lambda m, at: (clamped(m), 0)),
        pl.BlockSpec((ROWS, cols), lambda m, at: (0, 0)),
        pl.BlockSpec((ROWS, wide), lambda m, at: (clamped(m), at[0] ^ 2)),
        pl.BlockSpec((ROWS, wide), lambda m, at: (0, at[0] ^ 2)),
        pl.BlockSpec((ROWS, wide), lambda m, at: (0, at[0] ^ 3)),
    ]
    in_specs += [pl.BlockSpec(p.shape, lambda m, at: (0, 0)) for p in second]
    in_specs += [
        pl.BlockSpec((pl.Element(p.shape[0]), pl.Element(cols)), lambda m, at: (0, begin))
        for p in third
    ]
    return pl.pallas_call(
        kernel,
        grid_spec=pltpu.PrefetchScalarGridSpec(
            num_scalar_prefetch=1,
            grid=(steps + 1,),
            in_specs=in_specs,
            out_specs=pl.BlockSpec((ROWS, cols), lambda m, at: (m, 0)),
            scratch_shapes=[pltpu.VMEM((2 * wide, cols), BF)],
        ),
        out_shape=jax.ShapeDtypeStruct((rows + late.shape[0], cols), BF),
        compiler_params=pltpu.CompilerParams(
            dimension_semantics=("arbitrary",), vmem_limit_bytes=26 * 2**20
        ),
        cost_estimate=pl.CostEstimate(
            flops=3 * (rows + late.shape[0]) * wide * cols,
            bytes_accessed=8 * 2**20,
            transcendentals=0,
        ),
        name="project",
    )(place, acc_early, acc_late, early, late, late, *second, *third)


def output_projection(place, heads, weights, first, count, kind):
    sp = len(heads)
    tile = OUT_TILE

    def kernel(place_ref, *refs):
        ys, ws, (out, ordered) = refs[:sp], refs[sp : sp + 4], refs[sp + 4 :]
        s, c = place_ref[0], place_ref[2]
        n = pl.program_id(0)

        @pl.when(n == 0)
        def _():
            for k, y in enumerate(ys):
                ordered[(s ^ k) ^ (2 * c)] = y[...]

        total = None
        for j, w in enumerate(ws):
            lanes = slice((j % 2) * VDIM, (j % 2 + 1) * VDIM)
            for local in range(2):
                part = jnp.dot(
                    ordered[(j // 2) * 2 + local, :, lanes],
                    w[local * VDIM : (local + 1) * VDIM],
                    preferred_element_type=F32,
                )
                total = part if total is None else total + part
        out[...] = total.astype(out.dtype)

    whole = pl.BlockSpec((WINDOW, 2 * VDIM), lambda n: (0, 0))
    in_specs = [pl.BlockSpec(memory_space=pltpu.SMEM)] + [whole] * sp
    in_specs += [pl.BlockSpec((2 * VDIM, tile), lambda n: (0, n + first))] * 4
    operands = [place, *heads, *weights]
    return pl.pallas_call(
        kernel,
        grid=(count,),
        in_specs=in_specs,
        out_specs=pl.BlockSpec((WINDOW, tile), lambda n: (0, n)),
        out_shape=jax.ShapeDtypeStruct((WINDOW, count * tile), kind),
        scratch_shapes=[pltpu.VMEM((sp, WINDOW, 2 * VDIM), BF)],
        compiler_params=pltpu.CompilerParams(
            dimension_semantics=("arbitrary",), vmem_limit_bytes=16 * 2**20
        ),
        cost_estimate=pl.CostEstimate(
            flops=2 * WINDOW * 2048 * count * tile,
            bytes_accessed=2048 * count * tile * 2,
            transcendentals=0,
        ),
        name="output",
    )(*operands)


def chip_body(
    tokens,
    norm_gain,
    query_diff,
    key_diff,
    value_diff,
    lam,
    output_norm_gain,
    query_win,
    keyval_win,
    sink,
    proj_diff,
    proj_win,
):
    ng, sp, tp = (lax.axis_size(a) for a in AXES)
    nx = tp // 2
    g, s, t = (lax.axis_index(a) for a in AXES)
    x, c = t // 2, t % 2

    def send(value, target, only=None):
        pairs = []
        for i in range(ng * sp * tp):
            at = (i // (sp * tp), i // tp % sp, i % tp // 2, i % 2)
            if only is None or only(*at):
                a, b, d, e = target(*at)
                pairs.append((i, ((a * sp + b) * nx + d) * 2 + e))
        return lax.ppermute(value, AXES, pairs)

    def over_core(v):
        return send(v, lambda a, b, d, e: (a, b, d, e ^ 1))

    def over_x(v):
        return send(v, lambda a, b, d, e: (a, b, d ^ 1, e))

    def over_y(v):
        return send(v, lambda a, b, d, e: (a ^ 1, b, d, e))

    def over_z(v, k):
        return send(v, lambda a, b, d, e: (a, b ^ k, d, e))

    def mids(v, k):
        return send(v, lambda a, b, d, e: (a, b ^ k, d, e), lambda a, b, d, e: b in (1, 2))

    mid = (s == 1) | (s == 2)
    normed = root_mean_square_rows(tokens.astype(F32), norm_gain).astype(BF)
    one = over_z(normed, 1)
    near = mids(normed, 3)
    tx0 = over_x(normed)
    far = mids(near, 1)
    cross = mids(one, 3)
    tx1 = over_x(one)
    last = mids(cross, 1)
    slot2 = jnp.where(mid, cross, far)
    tx2 = over_x(slot2)
    slot3 = jnp.where(mid, near, last)
    tx3 = over_x(slot3)
    early = jnp.concatenate([normed, one, slot2, tx0, tx1, tx2], axis=0)
    late = jnp.concatenate([slot3, tx3], axis=0)

    rows_w = query_diff.shape[0]
    quarter = rows_w // 4

    def pack(lo, size, head):
        parts = []
        for w in (key_diff, value_diff, query_diff, query_win):
            parts.append(lax.dynamic_slice(w, (lo, head * VDIM), (size, VDIM)))
        return jnp.concatenate(parts, axis=1)

    def kv_pack(lo, size, h):
        kv = lax.dynamic_slice(keyval_win, (nx * x + h // 2, lo, 0), (1, size, 2 * HEAD))
        return kv[0]

    def with_kv(four, kv):
        return jnp.concatenate([four[:, : 2 * VDIM], kv, four[:, 2 * VDIM :]], axis=1)

    mine_lo = (g * 2 + c) * quarter
    give_lo = (g * 2 + 1 - c) * quarter
    give = jnp.stack([pack(give_lo, quarter, 0), pack(give_lo, quarter, 1)])
    keep = jnp.stack([pack(mine_lo, quarter, 0), pack(mine_lo, quarter, 1)])
    both = jnp.concatenate([keep, over_core(give)], axis=0)
    local = pack(0, rows_w, s % 2)
    moved = send(local, lambda a, b, d, e: (a, b, d, e ^ 1), lambda a, b, d, e: e == b // 2)
    own = with_kv(jnp.where(c == s // 2, local, moved), kv_pack(0, rows_w, s))

    place = jnp.stack([s, x, c, g]).astype(jnp.int32)

    def package(k):
        h = s ^ k
        pick = lax.dynamic_index_in_dim(both, ((h // 2) ^ c) * 2 + h % 2, 0, keepdims=False)
        return pick, kv_pack(mine_lo, quarter, h)

    def chunk(part, k):
        got = over_z(part, k)
        got_y = over_y(got)
        return [got, got_y, over_core(jnp.concatenate([got, got_y], axis=0))]

    w1 = chunk(with_kv(*package(1)), 1)
    w3 = chunk(with_kv(*package(3)), 3)
    four, kv = package(2)
    w2a = chunk(jnp.concatenate([four[:, : 2 * VDIM], kv], axis=1), 2)
    w2b = chunk(four[:, 2 * VDIM :], 2)
    split = 3 * VDIM
    first = [(0, [own]), (1, w1)]
    sums = project_sum(place, early, None, first, split)
    ends = project_sum(place, late, None, first, split)
    sums = project_sum(place, early, sums, [(3, w3)], split)
    kv_own = project_rest(place, early, late, sums[0], ends[0], w3, w2a, 0)
    kv_oth = over_core(kv_own)
    queries = project_rest(place, early, late, sums[1], ends[1], w3, w2b, split)

    scalars = (lam, over_core(lam), sink, over_core(sink))
    gain = output_norm_gain.reshape(1, VDIM)
    weights = [proj_diff, proj_win, over_core(proj_diff), over_core(proj_win)]

    def attend(flip, first, count):
        return attention(
            place, scalars, gain, queries, kv_own, kv_oth, nx, flip, first, count
        )

    high = [over_z(y, k) for k, y in zip((2, 3), attend(1, 2, sp - 2))]
    low = attend(1, 0, 2)
    far_heads = [low[0], over_z(low[1], 1), *high]
    y_near = attend(0, 0, sp)
    near_heads = [y_near[0]] + [over_z(y_near[k], k) for k in range(1, sp)]
    received = []
    tiles = proj_diff.shape[1] // OUT_TILE
    for begin, end in ((0, 1), (1, tiles // 2), (tiles // 2, tiles)):
        part = output_projection(place, far_heads, weights, begin, end - begin, BF)
        received.append(over_x(part))
    kept = output_projection(place, near_heads, weights, 0, tiles, F32)
    return (kept + jnp.concatenate(received, axis=1).astype(F32)).astype(BF)


def solution(mesh):
    placed = (
        P(("grp", "sp", "tp"), None),
        P(),
        P("sp", "tp"),
        P("sp", "tp"),
        P("sp", "tp"),
        P("tp"),
        P(),
        P("sp", "tp"),
        P(None, "sp", None),
        P("tp"),
        P("tp", None),
        P("tp", None),
    )
    sizes = dict(mesh.shape)

    def body(*args):
        tokens, lam, sink = args[0], args[5], args[9]
        fits = (
            sizes["grp"] == 2
            and sizes["sp"] == 4
            and sizes["tp"] == 4
            and tokens.shape[0] == WINDOW
            and lam.shape[0] == 2
            and sink.shape[0] == 4
        )
        return (chip_body if fits else general_body)(*args)

    return jax.shard_map(
        body, mesh=mesh, in_specs=placed, out_specs=P(("grp", "sp", "tp"), None), check_vma=False
    )
```
